512 devices in a mesh: ep: 128 (over z, x, core), tp: 4 (over y).
Axes of the slice: x: 4, y: 4, z: 16, core: 2. Of those that a mesh axis runs over, the one named last changes fastest.
Arguments:
- tokens: bfloat16 [6144, 2048], P('ep', 'tp'), may hold values from -6 to 6
- conv_state: bfloat16 [6144, 3, 1024], P('ep', None, 'tp'), may hold values from -6 to 6
- lru_state: float32 [6144, 1024], P('ep', 'tp'), may hold values from -6 to 6
- mix_gain: float32 [2048], replicated, may hold values from 0.1 to 1.9
- input_weight: bfloat16 [2048, 1024], P(None, 'tp'), may hold values from -0.125 to 0.125
- branch_weight: bfloat16 [2048, 1024], P(None, 'tp'), may hold values from -0.125 to 0.125
- conv_taps: float32 [4, 1024], P(None, 'tp'), may hold values from -3 to 3
- conv_bias: float32 [1024], P('tp'), may hold values from -3 to 3
- recur_weight: bfloat16 [8, 128, 128], P('tp'), may hold values from -0.5 to 0.5
- recur_bias: float32 [1024], P('tp'), may hold values from -4 to 4
- inject_weight: bfloat16 [8, 128, 128], P('tp'), may hold values from -0.5 to 0.5
- inject_bias: float32 [1024], P('tp'), may hold values from -4 to 4
- decay_param: float32 [1024], P('tp'), may hold values from -1 to 4
- output_weight: bfloat16 [1024, 2048], P(None, 'tp'), may hold values from -0.1875 to 0.1875
- moe_gain: float32 [2048], replicated, may hold values from 0.1 to 1.9
- route_ids: int32 [6144, 2], P('ep'), may hold values from 0 to 127, as said below
- route_logits: float32 [6144, 2], P('ep'), may hold values from -6 to 6
- group_weight: float32 [6144], P('ep'), may hold values from 0.25 to 1
- expert_gate: bfloat16 [128, 2048, 512], P('ep', None, 'tp'), may hold values from -0.125 to 0.125
- expert_up: bfloat16 [128, 2048, 512], P('ep', None, 'tp'), may hold values from -0.125 to 0.125
- expert_down: bfloat16 [128, 512, 2048], P('ep', 'tp'), may hold values from -0.25 to 0.25
Outputs:
- result: bfloat16 [6144, 2048], P('ep', 'tp')
- new_state: float32 [6144, 1024], P('ep', 'tp')
- new_conv: bfloat16 [6144, 3, 1024], P('ep', None, 'tp')
The draws below stay inside these ranges and needn't reach their ends.
Inputs may be any that keep to these rules, and one draw needn't show every extreme that they name: `route_ids`: each row names 2 different experts of one group of 4 consecutive experts (the group of expert e is e // 4). In each aligned block of 48 rows no expert is named by more than 2 rows, and in every draw some expert is named by exactly 2 rows of every block.
All inputs are finite; a program needn't handle non-finite values.
Results may differ from the reference program's by a relative error of at most 0.013.
Values may be sent and summed in bfloat16 or wider, within the bound.
No kernel may reach another device: no remote copies, remote signals or barrier semaphores. Data moves between devices by JAX's collectives and lax.ppermute only.
A program may use at most 64 MiB of HBM per device.

```python
import jax
import jax.numpy as jnp
from jax import lax

D = 2048
LRU_W = 1024
LRU_BLOCKS = 8
BW = 128
TAPS = 4
FF = 512
FF_BLK = 128
PER_GROUP = 4
TOPK = 2
SEQ_GRP = 48
EXPERTS = 128
CAP = 2
BATCH = 6144


def draw_route_ids(key, part):
    groups = EXPERTS // PER_GROUP
    reach = PER_GROUP * CAP // TOPK
    slot_total = groups * reach
    group_of = jnp.repeat(jnp.arange(groups, dtype=jnp.int32), reach)
    rank_of = jnp.tile(jnp.arange(reach, dtype=jnp.int32), groups)
    base_key = jax.random.fold_in(key, 17)
    hot_group = jax.random.randint(jax.random.fold_in(base_key, 1), (), 0, groups)
    levels = jax.random.randint(jax.random.fold_in(base_key, 2), (groups,), 0, 4) * 2 ** 16
    column = jnp.arange(groups, dtype=jnp.int32)[:, None] * PER_GROUP + jnp.arange(PER_GROUP, dtype=jnp.int32)[None, :]

    def one_block(block_num, block_key):
        noise_key, perm_key, order_key = jax.random.split(block_key, 3)
        near = (block_num + 1) % EXPERTS
        far = (block_num + EXPERTS // 2) % EXPERTS
        forced = ((group_of == near // PER_GROUP) | (group_of == far // PER_GROUP)) & (rank_of == 0)
        noise = jax.random.randint(noise_key, (slot_total,), 0, 2 ** 16)
        priority = noise + levels[group_of] + jnp.where(group_of == hot_group, 2 ** 18, 0) + jnp.where(forced, 2 ** 19, 0)
        distinct = priority * slot_total + jnp.arange(slot_total, dtype=jnp.int32)
        order = jnp.argsort(-distinct)
        chosen = order[:SEQ_GRP]
        chosen_group = group_of[chosen]
        chosen_rank = rank_of[chosen]
        local_noise = jax.random.randint(perm_key, (groups, PER_GROUP), 0, 2 ** 10) * PER_GROUP + jnp.arange(PER_GROUP, dtype=jnp.int32)[None, :]
        local_noise = jnp.where(column == near, -2, jnp.where(column == far, -1, local_noise))
        arrange = jnp.argsort(local_noise, axis=1).astype(jnp.int32)
        position = (chosen_rank[:, None] * TOPK + jnp.arange(TOPK, dtype=jnp.int32)[None, :]) % PER_GROUP
        local = jnp.take_along_axis(arrange[chosen_group], position, axis=1)
        expert_ids = chosen_group[:, None] * PER_GROUP + local
        shuffle = jax.random.permutation(order_key, SEQ_GRP)
        return expert_ids[shuffle]
    block_keys = jax.random.split(base_key, EXPERTS)
    drawn = jax.vmap(one_block)(jnp.arange(EXPERTS, dtype=jnp.int32), block_keys)
    return drawn.reshape(SEQ_GRP * EXPERTS, TOPK).astype(jnp.int32)


def block_levels(stream_key, extent, cuts, low, top_value):
    level, own = 1.0, jax.random.fold_in(stream_key, 6)
    for axis_at, shards_of in cuts:
        draws = jnp.exp(jax.random.uniform(jax.random.fold_in(own, axis_at), (shards_of,), jnp.float32, low / len(cuts), top_value / len(cuts)))
        level = level * jnp.repeat(draws, extent[axis_at] // shards_of).reshape([-1 if axis == axis_at else 1 for axis in range(len(extent))])
    return level


def centred(key, extent, deviation, most, cuts=(), kind=jnp.bfloat16):
    values = deviation * jax.random.normal(key, extent, jnp.float32)
    if cuts:
        values = values * block_levels(key, extent, cuts, -0.22, 0.18)
    return jnp.clip(values, -most, most).astype(kind)


def setup_inputs(seed: int = 0) -> dict:
    streams_of = jax.random.split(jax.random.key(seed), 22)
    return {
        "tokens": centred(streams_of[0], (BATCH, D), 1.0, 6.0, ((0, 128), (1, 4))),
        "conv_state": centred(streams_of[1], (BATCH, TAPS - 1, LRU_W), 1.0, 6.0, ((0, 128), (2, 4))),
        "lru_state": centred(streams_of[2], (BATCH, LRU_W), 1.0, 6.0, ((0, 128), (1, 4)), jnp.float32),
        "mix_gain": jnp.clip(1.0 + 0.18 * jax.random.normal(streams_of[3], (D,), jnp.float32), 0.1, 1.9),
        "input_weight": centred(streams_of[4], (D, LRU_W), D ** -0.5, 0.125, ((1, 4),)),
        "branch_weight": centred(streams_of[5], (D, LRU_W), D ** -0.5, 0.125, ((1, 4),)),
        "conv_taps": centred(streams_of[6], (TAPS, LRU_W), 0.5, 3.0, ((1, 4),), jnp.float32),
        "conv_bias": centred(streams_of[7], (LRU_W,), 0.5, 3.0, ((0, 4),), jnp.float32),
        "recur_weight": centred(streams_of[8], (LRU_BLOCKS, BW, BW), BW ** -0.5, 0.5, ((0, 4),)),
        "recur_bias": centred(streams_of[9], (LRU_W,), 1.0, 4.0, ((0, 4),), jnp.float32),
        "inject_weight": centred(streams_of[10], (LRU_BLOCKS, BW, BW), BW ** -0.5, 0.5, ((0, 4),)),
        "inject_bias": centred(streams_of[11], (LRU_W,), 1.0, 4.0, ((0, 4),), jnp.float32),
        "decay_param": jnp.clip(-1.0 + 5.0 * jax.random.uniform(streams_of[12], (LRU_W,), jnp.float32) ** block_levels(streams_of[12], (LRU_W,), ((0, 4),), -0.2, 0.2), -1.0, 4.0),
        "output_weight": centred(streams_of[13], (LRU_W, D), LRU_W ** -0.5, 0.1875, ((1, 4),)),
        "moe_gain": jnp.clip(1.0 + 0.18 * jax.random.normal(streams_of[14], (D,), jnp.float32), 0.1, 1.9),
        "route_ids": draw_route_ids(jax.random.fold_in(streams_of[21], 71), 0),
        "route_logits": centred(streams_of[16], (BATCH, TOPK), 1.0, 6.0, ((0, 128),), jnp.float32),
        "group_weight": jnp.clip(0.25 + 0.75 * jax.random.uniform(streams_of[17], (BATCH,), jnp.float32) ** block_levels(streams_of[17], (BATCH,), ((0, 128),), -0.2, 0.2), 0.25, 1.0),
        "expert_gate": centred(streams_of[18], (EXPERTS, D, FF), D ** -0.5, 0.125, ((0, 128), (2, 4))),
        "expert_up": centred(streams_of[19], (EXPERTS, D, FF), D ** -0.5, 0.125, ((0, 128), (2, 4))),
        "expert_down": centred(streams_of[20], (EXPERTS, FF, D), FF ** -0.5, 0.25, ((0, 128), (1, 4))),
    }


EPS = 1e-06
RATE = 8.0

def rms_norm(values, scales):
    wide = values.astype(jnp.float32)
    return wide * lax.rsqrt(lax.optimization_barrier(jnp.mean(wide * wide, axis=-1, keepdims=True)) + EPS) * scales

def block_gate(signal, weight, bias):
    blocks = weight.shape[0]
    grouped = signal.astype(jnp.float32).reshape(signal.shape[0], blocks, -1)
    mixed_out = jnp.einsum('sbi,bij->sbj', grouped, weight.astype(jnp.float32)).reshape(signal.shape[0], -1)
    return jax.nn.sigmoid(mixed_out + bias)

def expert_mix(moe_in, route_ids, route_logits, group_weight, expert_gate, expert_up, expert_down):
    row_total = moe_in.shape[0]
    blocks = row_total // SEQ_GRP
    experts = expert_gate.shape[0]
    flat_ids = route_ids.reshape(blocks, SEQ_GRP * TOPK)
    one_hot = (flat_ids[:, :, None] == jnp.arange(experts, dtype=jnp.int32)[None, None, :]).astype(jnp.int32)
    earlier = jnp.cumsum(one_hot, axis=1) - one_hot
    slot_rank = lax.optimization_barrier(jnp.sum(one_hot * earlier, axis=2))
    block_num = jnp.arange(blocks, dtype=jnp.int32)[:, None]
    slot_index = (flat_ids * (blocks * CAP) + block_num * CAP + slot_rank).reshape(-1).astype(jnp.int32)
    source = jnp.repeat(jnp.arange(row_total, dtype=jnp.int32), TOPK)
    raised = jnp.exp(route_logits)
    route_weight = group_weight[:, None] * raised / lax.optimization_barrier(jnp.sum(raised, axis=1, keepdims=True))
    row_table = jnp.zeros((experts * blocks * CAP,), jnp.int32).at[slot_index].set(source)
    weight_table = jnp.zeros((experts * blocks * CAP,), jnp.float32).at[slot_index].set(route_weight.reshape(-1))
    row_table = row_table.reshape(experts, blocks * CAP)
    weight_table = weight_table.reshape(experts, blocks * CAP)

    def visit(running, members):
        row_index, factor, gate_mat, up_mat, down_mat = members
        picked = jnp.take(moe_in, row_index, axis=0)
        gate_act = jnp.dot(picked, gate_mat, preferred_element_type=jnp.float32)
        up_act = jnp.dot(picked, up_mat, preferred_element_type=jnp.float32)
        hidden = (jax.nn.silu(gate_act) * up_act).astype(jnp.bfloat16)
        summed = jnp.zeros((picked.shape[0], moe_in.shape[1]), jnp.float32)
        for part_num in range(FF // FF_BLK):
            partial_value = jnp.dot(hidden[:, part_num * FF_BLK:(part_num + 1) * FF_BLK], down_mat[part_num * FF_BLK:(part_num + 1) * FF_BLK], preferred_element_type=jnp.float32)
            summed = summed + lax.optimization_barrier(partial_value.astype(jnp.bfloat16)).astype(jnp.float32)
        outcome = lax.optimization_barrier(summed.astype(jnp.bfloat16)).astype(jnp.float32)
        return (running.at[row_index].add(factor[:, None] * outcome), None)
    start_total = jnp.zeros((row_total, moe_in.shape[1]), jnp.float32)
    running, unused = lax.scan(visit, start_total, (row_table, weight_table, expert_gate, expert_up, expert_down))
    return running

def reference(tokens, conv_state, lru_state, mix_gain, input_weight, branch_weight, conv_taps, conv_bias, recur_weight, recur_bias, inject_weight, inject_bias, decay_param, output_weight, moe_gain, route_ids, route_logits, group_weight, expert_gate, expert_up, expert_down):
    normed = rms_norm(tokens, mix_gain).astype(jnp.bfloat16)
    branch_x = jnp.dot(normed, input_weight, preferred_element_type=jnp.float32).astype(jnp.bfloat16)
    branch_g = jnp.dot(normed, branch_weight, preferred_element_type=jnp.float32).astype(jnp.bfloat16)
    window = jnp.concatenate([conv_state, branch_x[:, None, :]], axis=1)
    conv_sum = conv_bias + lax.optimization_barrier(jnp.sum(window.astype(jnp.float32) * conv_taps[None], axis=1))
    conv_out = conv_sum.astype(jnp.bfloat16)
    recur_gate = block_gate(conv_out, recur_weight, recur_bias)
    inject_gate = block_gate(conv_out, inject_weight, inject_bias)
    log_rate = -RATE * recur_gate * jax.nn.softplus(-decay_param)
    new_state = jnp.exp(log_rate) * lru_state + jnp.sqrt(-jnp.expm1(2.0 * log_rate)) * inject_gate * conv_out.astype(jnp.float32)
    mixer_out = (new_state * jax.nn.gelu(branch_g.astype(jnp.float32))).astype(jnp.bfloat16)
    mixed_out = jnp.dot(mixer_out, output_weight, preferred_element_type=jnp.float32)
    stream = (tokens.astype(jnp.float32) + mixed_out).astype(jnp.bfloat16)
    moe_in = rms_norm(stream, moe_gain).astype(jnp.bfloat16)
    routed = expert_mix(moe_in, route_ids, route_logits, group_weight, expert_gate, expert_up, expert_down)
    result = (stream.astype(jnp.float32) + routed).astype(jnp.bfloat16)
    return (result, new_state, window[:, 1:])
```

```python
import jax
import jax.numpy as jnp
from jax import lax
from jax.sharding import PartitionSpec as P

PER_GROUP = 4
EPS = 1e-06
RATE = 8.0
F32 = jnp.float32
BF16 = jnp.bfloat16


def to_each(value, axis):
    size = lax.axis_size(axis)
    return lax.all_to_all(
        jnp.broadcast_to(value[None], (size, *value.shape)), axis, 0, 0, tiled=True
    )


def side_by_side(parts):
    size, rows, width = parts.shape
    return jnp.swapaxes(parts, 0, 1).reshape(rows, size * width)


def dot(a, b):
    return jnp.dot(a, b, preferred_element_type=F32)


def block_gate(signal, weight, bias):
    blocks = weight.shape[0]
    grouped = signal.reshape(signal.shape[0], blocks, -1)
    mixed_out = jnp.einsum("sbi,bij->sbj", grouped, weight, preferred_element_type=F32)
    return jax.nn.sigmoid(mixed_out.reshape(signal.shape[0], -1) + bias)


def body(
    tokens,
    conv_state,
    lru_state,
    mix_gain,
    input_weight,
    branch_weight,
    conv_taps,
    conv_bias,
    recur_weight,
    recur_bias,
    inject_weight,
    inject_bias,
    decay_param,
    output_weight,
    moe_gain,
    route_ids,
    route_logits,
    group_weight,
    expert_gate,
    expert_up,
    expert_down,
):
    seq_count, quarter = tokens.shape
    members = lax.axis_size("tp")
    model_width = members * quarter
    experts = lax.axis_size("ep")
    top_count = route_ids.shape[1]
    capacity = 2

    flat_ids = route_ids.reshape(-1)
    one_hot = (flat_ids[:, None] == jnp.arange(experts, dtype=jnp.int32)[None, :]).astype(jnp.int32)
    earlier = jnp.cumsum(one_hot, axis=0) - one_hot
    slot_rank = jnp.sum(one_hot * earlier, axis=1).reshape(seq_count, top_count)
    slot_index = route_ids * capacity + slot_rank
    slots = experts * capacity
    targets = jnp.arange(slots, dtype=jnp.int32)
    hits = (targets[None, None, :] == slot_index[:, :, None])
    dispatch = jnp.any(targets[:, None, None] == slot_index[None], axis=2).astype(BF16)
    raised = jnp.exp(route_logits)
    route_weight = group_weight[:, None] * raised / jnp.sum(raised, axis=1, keepdims=True)
    combine = jnp.sum(jnp.where(hits, route_weight[:, :, None], 0.0), axis=1)
    combine_high = combine.astype(BF16)
    combine_low = (combine - combine_high.astype(F32)).astype(BF16)

    wide = to_each(tokens, "tp").astype(F32)
    scale = lax.rsqrt(jnp.sum(wide * wide, axis=(0, 2)) / model_width + EPS)
    normed = (
        wide * scale[None, :, None] * mix_gain.reshape(members, 1, quarter)
    ).astype(BF16)
    normed = side_by_side(normed)
    branch_x = dot(normed, input_weight).astype(BF16)
    branch_g = dot(normed, branch_weight).astype(BF16)
    window = jnp.concatenate([conv_state, branch_x[:, None, :]], axis=1)
    conv_sum = conv_bias + jnp.sum(window.astype(F32) * conv_taps[None], axis=1)
    conv_out = conv_sum.astype(BF16)
    recur_gate = block_gate(conv_out, recur_weight, recur_bias)
    inject_gate = block_gate(conv_out, inject_weight, inject_bias)
    log_rate = -RATE * recur_gate * jax.nn.softplus(-decay_param)
    new_state = jnp.exp(log_rate) * lru_state + jnp.sqrt(
        -jnp.expm1(2.0 * log_rate)
    ) * inject_gate * conv_out.astype(F32)
    mixer_out = (new_state * jax.nn.gelu(branch_g.astype(F32))).astype(BF16)
    mixed_out = dot(side_by_side(to_each(mixer_out, "tp")), output_weight)
    stream = (tokens.astype(F32) + mixed_out).astype(BF16)

    outgoing = dot(dispatch, stream).astype(BF16)
    arrived = lax.all_to_all(outgoing, "ep", 0, 0, tiled=True)
    rows = to_each(arrived, "tp").astype(F32)
    row_scale = lax.rsqrt(jnp.sum(rows * rows, axis=(0, 2)) / model_width + EPS)
    moe_in = (
        rows * row_scale[None, :, None] * moe_gain.reshape(members, 1, quarter)
    ).astype(BF16)
    moe_in = side_by_side(moe_in)
    gate_act = dot(moe_in, expert_gate[0])
    up_act = dot(moe_in, expert_up[0])
    hidden = (jax.nn.silu(gate_act) * up_act).astype(BF16)
    down = expert_down[0]
    partial_out = jnp.concatenate(
        [
            dot(hidden, down[:, m * quarter : (m + 1) * quarter]).astype(BF16)
            for m in range(members)
        ],
        axis=0,
    )
    partial_in = lax.all_to_all(partial_out, "tp", 0, 0, tiled=True)
    answer = jnp.sum(partial_in.reshape(members, slots, quarter).astype(F32), axis=0).astype(BF16)
    returned = lax.all_to_all(answer, "ep", 0, 0, tiled=True)
    routed = dot(combine_high, returned) + dot(combine_low, returned)
    result = (stream.astype(F32) + routed).astype(BF16)
    return (result, new_state, window[:, 1:])


def solution(mesh):
    in_specs = (
        P("ep", "tp"),
        P("ep", None, "tp"),
        P("ep", "tp"),
        P(),
        P(None, "tp"),
        P(None, "tp"),
        P(None, "tp"),
        P("tp"),
        P("tp", None, None),
        P("tp"),
        P("tp", None, None),
        P("tp"),
        P("tp"),
        P(None, "tp"),
        P(),
        P("ep", None),
        P("ep", None),
        P("ep"),
        P("ep", None, "tp"),
        P("ep", None, "tp"),
        P("ep", "tp", None),
    )
    out_specs = (P("ep", "tp"), P("ep", "tp"), P("ep", None, "tp"))
    return jax.shard_map(body, mesh=mesh, in_specs=in_specs, out_specs=out_specs, check_vma=False)
```

```python
import jax
import jax.numpy as jnp
from jax import lax
from jax.experimental import pallas as pl
from jax.experimental.pallas import tpu as pltpu
from jax.sharding import PartitionSpec as P

EPS = 1e-06
RATE = 8.0
F32 = jnp.float32
BF16 = jnp.bfloat16


def to_each(value, axis):
    size = lax.axis_size(axis)
    return lax.all_to_all(
        jnp.broadcast_to(value[None], (size, *value.shape)), axis, 0, 0, tiled=True
    )


def side_by_side(parts):
    size, rows, width = parts.shape
    return jnp.swapaxes(parts, 0, 1).reshape(rows, size * width)


def dot(a, b):
    return jnp.dot(a, b, preferred_element_type=F32)


VMEM = pl.BlockSpec(memory_space=pltpu.VMEM)
SUM_ROWS = 16


def call(kernel, shape, count):
    return pl.pallas_call(
        kernel,
        out_shape=pltpu.VMEM(shape, BF16),
        in_specs=[pl.BlockSpec(memory_space=pltpu.SMEM)] + [VMEM] * count,
        out_specs=VMEM,
    )


def near(value):
    return pltpu.with_memory_space_constraint(value, pltpu.VMEM)


def first_products(member_ref, rows_ref, gain_ref, *refs):
    *weight_refs, out_ref = refs
    members = len(weight_refs)
    rows = rows_ref[...].astype(F32)
    count, width = rows.shape
    half = width // 2
    scaled = (rows * gain_ref[...]).astype(BF16)
    for k, weight_ref in enumerate(weight_refs):
        product = dot(scaled[:, :half], weight_ref[:half, :half]) + dot(
            scaled[:, half:], weight_ref[:half, half:]
        )
        owner = lax.rem(member_ref[0] + (members - k), members)
        out_ref[owner, :count, :] = product.astype(BF16)
    squares = rows * rows
    high = squares.astype(BF16)
    low = (squares - high.astype(F32)).astype(BF16)
    ones = jnp.ones((SUM_ROWS, width), BF16)
    across = (((1,), (1,)), ((), ()))
    sums = lax.dot_general(ones, high, across, preferred_element_type=F32) + lax.dot_general(
        ones, low, across, preferred_element_type=F32
    )
    sums_high = sums.astype(BF16)
    sums_low = (sums - sums_high.astype(F32)).astype(BF16)
    place = lax.broadcasted_iota(jnp.int32, sums.shape, 0)
    mixed = jnp.where(
        place == 0,
        sums_high.astype(F32),
        jnp.where(place == 1, sums_low.astype(F32), 0.0),
    ).astype(BF16)
    for k in range(members):
        out_ref[k, count:, :] = mixed


def hidden_units(member_ref, parts_ref, out_ref):
    members, total, width = parts_ref.shape
    count = total - SUM_ROWS
    half = width // 2
    product = parts_ref[0, :count, :].astype(F32)
    sums = parts_ref[0, count:, :].astype(F32)
    for k in range(1, members):
        product = product + parts_ref[k, :count, :].astype(F32)
        sums = sums + parts_ref[k, count:, :].astype(F32)
    row_sum = jnp.sum(jnp.transpose(sums), axis=1, keepdims=True)
    product = product * lax.rsqrt(row_sum / (members * 512) + EPS)
    gate = product[:, :half]
    hidden = (gate * jax.nn.sigmoid(gate) * product[:, half:]).astype(BF16)
    for k in range(members):
        out_ref[k] = hidden


def last_product(member_ref, hidden_ref, *refs):
    *weight_refs, out_ref = refs
    members, _, width = hidden_ref.shape
    total = jnp.zeros(out_ref.shape, F32)
    for k, weight_ref in enumerate(weight_refs):
        owner = lax.rem(member_ref[0] + (members - k), members)
        total = total + dot(hidden_ref[owner], weight_ref[weight_ref.shape[0] - width :, :])
    out_ref[...] = total.astype(BF16)


def block_gate(signal, weight, bias):
    blocks = weight.shape[0]
    grouped = signal.reshape(signal.shape[0], blocks, -1)
    mixed_out = jnp.einsum("sbi,bij->sbj", grouped, weight, preferred_element_type=F32)
    return jax.nn.sigmoid(mixed_out.reshape(signal.shape[0], -1) + bias)


def body(
    tokens,
    conv_state,
    lru_state,
    mix_gain,
    input_weight,
    branch_weight,
    conv_taps,
    conv_bias,
    recur_weight,
    recur_bias,
    inject_weight,
    inject_bias,
    decay_param,
    output_weight,
    moe_gain,
    route_ids,
    route_logits,
    group_weight,
    expert_gate,
    expert_up,
    expert_down,
):
    seq_count, quarter = tokens.shape
    members = lax.axis_size("tp")
    model_width = members * quarter
    experts = lax.axis_size("ep")
    member = lax.axis_index("tp")
    top_count = route_ids.shape[1]
    capacity = 2

    flat_ids = route_ids.reshape(-1)
    one_hot = (flat_ids[:, None] == jnp.arange(experts, dtype=jnp.int32)[None, :]).astype(jnp.int32)
    earlier = jnp.cumsum(one_hot, axis=0) - one_hot
    slot_rank = jnp.sum(one_hot * earlier, axis=1).reshape(seq_count, top_count)
    slot_index = route_ids * capacity + slot_rank
    slots = experts * capacity
    targets = jnp.arange(slots, dtype=jnp.int32)
    hits = (targets[None, None, :] == slot_index[:, :, None])
    dispatch = jnp.any(targets[:, None, None] == slot_index[None], axis=2).astype(BF16)
    raised = jnp.exp(route_logits)
    route_weight = group_weight[:, None] * raised / jnp.sum(raised, axis=1, keepdims=True)
    combine = jnp.sum(jnp.where(hits, route_weight[:, :, None], 0.0), axis=1)
    combine_high = combine.astype(BF16)
    combine_low = (combine - combine_high.astype(F32)).astype(BF16)

    wide = to_each(tokens, "tp").astype(F32)
    scale = lax.rsqrt(jnp.sum(wide * wide, axis=(0, 2)) / model_width + EPS)
    normed = (
        wide * scale[None, :, None] * mix_gain.reshape(members, 1, quarter)
    ).astype(BF16)
    normed = side_by_side(normed)
    branch_x = dot(normed, input_weight).astype(BF16)
    branch_g = dot(normed, branch_weight).astype(BF16)
    window = jnp.concatenate([conv_state, branch_x[:, None, :]], axis=1)
    conv_sum = conv_bias + jnp.sum(window.astype(F32) * conv_taps[None], axis=1)
    conv_out = conv_sum.astype(BF16)
    recur_gate = block_gate(conv_out, recur_weight, recur_bias)
    inject_gate = block_gate(conv_out, inject_weight, inject_bias)
    log_rate = -RATE * recur_gate * jax.nn.softplus(-decay_param)
    new_state = jnp.exp(log_rate) * lru_state + jnp.sqrt(
        -jnp.expm1(2.0 * log_rate)
    ) * inject_gate * conv_out.astype(F32)
    mixer_out = (new_state * jax.nn.gelu(branch_g.astype(F32))).astype(BF16)
    mixer_copies = jnp.broadcast_to(mixer_out[None], (members, *mixer_out.shape))

    gate_cut = expert_gate[0].reshape(members, 2, quarter // 2, -1)
    up_cut = expert_up[0].reshape(members, 2, quarter // 2, -1)
    down = expert_down[0]
    down_cut = jnp.stack([down[:, m * quarter : (m + 1) * quarter] for m in range(members)])
    cut = jnp.concatenate(
        [
            jnp.concatenate(
                [gate_cut[:, 0], up_cut[:, 0], gate_cut[:, 1], up_cut[:, 1]], axis=2
            ),
            down_cut,
        ],
        axis=1,
    )
    gain_part = lax.dynamic_slice_in_dim(moe_gain, member * quarter, quarter, 0)[None]
    cuts = [
        lax.dynamic_index_in_dim(cut, lax.rem(member + k, members), 0, keepdims=False)
        for k in range(members)
    ]
    mixer_copies, cuts, combine_high, combine_low, dispatch = lax.optimization_barrier(
        (mixer_copies, cuts, combine_high, combine_low, dispatch)
    )
    mixer_parts = lax.all_to_all(mixer_copies, "tp", 0, 0, tiled=True)
    weights = [cuts[0]]
    for k in range(1, members):
        ring = [(m, (m + k) % members) for m in range(members)]
        weights.append(lax.ppermute(cuts[k], "tp", ring))
    mixed_out = dot(side_by_side(mixer_parts), output_weight)
    stream = (tokens.astype(F32) + mixed_out).astype(BF16)

    outgoing = dot(dispatch, stream).astype(BF16)
    arrived = lax.all_to_all(outgoing, "ep", 0, 0, tiled=True)
    weights = [near(w) for w in weights]
    place = member.astype(jnp.int32)[None]
    products = call(first_products, (members, slots + SUM_ROWS, 256), members + 2)(
        place, near(arrived), near(gain_part), *weights
    )
    products = lax.all_to_all(products, "tp", 0, 0, tiled=True)
    hidden = call(hidden_units, (members, slots, 128), 1)(place, near(products))
    hidden = lax.all_to_all(hidden, "tp", 0, 0, tiled=True)
    answer = call(last_product, (slots, quarter), members + 1)(place, near(hidden), *weights)
    returned = lax.all_to_all(answer, "ep", 0, 0, tiled=True)
    routed = dot(combine_high, returned) + dot(combine_low, returned)
    result = (stream.astype(F32) + routed).astype(BF16)
    return (result, new_state, window[:, 1:])


def solution(mesh):
    in_specs = (
        P("ep", "tp"),
        P("ep", None, "tp"),
        P("ep", "tp"),
        P(),
        P(None, "tp"),
        P(None, "tp"),
        P(None, "tp"),
        P("tp"),
        P("tp", None, None),
        P("tp"),
        P("tp", None, None),
        P("tp"),
        P("tp"),
        P(None, "tp"),
        P(),
        P("ep", None),
        P("ep", None),
        P("ep"),
        P("ep", None, "tp"),
        P("ep", None, "tp"),
        P("ep", "tp", None),
    )
    out_specs = (P("ep", "tp"), P("ep", "tp"), P("ep", None, "tp"))
    return jax.shard_map(body, mesh=mesh, in_specs=in_specs, out_specs=out_specs, check_vma=False)
```

```python
import jax
import jax.numpy as jnp
from jax import lax
from jax.experimental import pallas as pl
from jax.experimental.pallas import tpu as pltpu
from jax.sharding import PartitionSpec as P

EPS = 1e-06
RATE = 8.0
CAPACITY = 2
SUM_ROWS = 16
F32 = jnp.float32
BF16 = jnp.bfloat16
VMEM = pl.BlockSpec(memory_space=pltpu.VMEM)
SMEM = pl.BlockSpec(memory_space=pltpu.SMEM)


def near(value):
    return pltpu.with_memory_space_constraint(value, pltpu.VMEM)


def call(kernel, outs, *args, scalar=None):
    scalars = () if scalar is None else (scalar,)
    return pl.pallas_call(
        kernel,
        out_shape=outs,
        in_specs=[SMEM] * len(scalars) + [VMEM] * len(args),
        out_specs=jax.tree.map(lambda _: VMEM, outs),
    )(*scalars, *args)


def dot(a, b):
    return jnp.dot(a, b, preferred_element_type=F32)


def dot_on(a, b, a_dim, b_dim):
    return lax.dot_general(a, b, (((a_dim,), (b_dim,)), ((), ())), preferred_element_type=F32)


def halves(value):
    high = value.astype(BF16)
    return high, (value - high.astype(F32)).astype(BF16)


def places(ids_ref, count, slots):
    ids = ids_ref[...]
    column = lax.broadcasted_iota(jnp.int32, (count, slots), 1)
    expert = lax.div(column, CAPACITY)
    place = lax.rem(column, CAPACITY)
    first = ids[:, 0:1] == expert
    second = ids[:, 1:2] == expert
    named = jnp.where(first | second, 1.0, 0.0)
    below = lax.broadcasted_iota(jnp.int32, (count, count), 1) < lax.broadcasted_iota(
        jnp.int32, (count, count), 0
    )
    earlier = dot(jnp.where(below, 1.0, 0.0).astype(BF16), named.astype(BF16))
    return jnp.where(earlier == place.astype(F32), named, 0.0), first


def dispatch_table(ids_ref, out_ref):
    out_ref[...] = places(ids_ref, *out_ref.shape)[0].astype(BF16)


def combine_tables(ids_ref, logits_ref, group_ref, high_ref, low_ref):
    hit, first = places(ids_ref, *high_ref.shape)
    raised = jnp.exp(logits_ref[...])
    weight = group_ref[...] * raised / (raised[:, 0:1] + raised[:, 1:2])
    high, low = halves(hit * jnp.where(first, weight[:, 0:1], weight[:, 1:2]))
    high_ref[...] = high
    low_ref[...] = low


def cut_weights(member_ref, gate_ref, up_ref, down_ref, *refs):
    *out_refs, done = refs
    members = len(out_refs)
    quarter = gate_ref.shape[1] // members
    half = quarter // 2
    width = gate_ref.shape[2]
    copies = []
    for k, out_ref in enumerate(out_refs):
        target = lax.rem(member_ref[0] + k, members)
        top = pl.multiple_of(target * quarter, quarter)
        pairs = [(down_ref.at[0, :, pl.ds(top, quarter)], out_ref.at[pl.ds(half, width), :])]
        for part in range(2):
            rows = pl.ds(pl.multiple_of(top + part * half, half), half)
            at = part * 2 * width
            into = [out_ref.at[pl.ds(0, half), pl.ds(at + j * width, width)] for j in range(2)]
            pairs += [(gate_ref.at[0, rows, :], into[0]), (up_ref.at[0, rows, :], into[1])]
        copies += [
            pltpu.make_async_copy(source, into, done.at[k, j])
            for j, (source, into) in enumerate(pairs)
        ]
    for copy in copies:
        copy.start()
    for copy in copies:
        copy.wait()


def block_gate(signal, weight, bias):
    blocks = weight.shape[0]
    grouped = signal.reshape(signal.shape[0], blocks, -1)
    mixed_out = jnp.einsum("sbi,bij->sbj", grouped, weight, preferred_element_type=F32)
    return jax.nn.sigmoid(mixed_out.reshape(signal.shape[0], -1) + bias)


def side_by_side(parts):
    size, rows, width = parts.shape
    return jnp.swapaxes(parts, 0, 1).reshape(rows, size * width)


def first_products(member_ref, rows_ref, gain_ref, weight_ref, out_ref, down_ref):
    members = weight_ref.shape[0]
    rows = rows_ref[...].astype(F32)
    count, width = rows.shape
    half = width // 2
    scaled = (rows * gain_ref[...]).astype(BF16)
    squares = rows * rows
    high, low = halves(squares)
    ones = jnp.ones((SUM_ROWS, width), BF16)
    sums_high, sums_low = halves(dot_on(ones, high, 1, 1) + dot_on(ones, low, 1, 1))
    place = lax.broadcasted_iota(jnp.int32, (SUM_ROWS, count), 0)
    sums = jnp.where(
        place == 0, sums_high.astype(F32), jnp.where(place == 1, sums_low.astype(F32), 0.0)
    ).astype(BF16)
    for k in range(members):
        product = dot(scaled[:, :half], weight_ref[k, :half, :half]) + dot(
            scaled[:, half:], weight_ref[k, :half, half:]
        )
        owner = lax.rem(member_ref[0] + (members - k), members)
        out_ref[owner, :count, :] = product.astype(BF16)
        out_ref[owner, count:, :] = sums
        down_ref[owner] = weight_ref[k, half:, :]


def hidden_units(parts_ref, out_ref):
    members, total, width = parts_ref.shape
    count = total - SUM_ROWS
    half = width // 2
    product = parts_ref[0, :count, :].astype(F32)
    sums = parts_ref[0, count:, :].astype(F32)
    for k in range(1, members):
        product = product + parts_ref[k, :count, :].astype(F32)
        sums = sums + parts_ref[k, count:, :].astype(F32)
    row_sum = jnp.sum(jnp.transpose(sums), axis=1, keepdims=True)
    product = product * lax.rsqrt(row_sum / (members * 2 * width) + EPS)
    gate = product[:, :half]
    hidden = (gate * jax.nn.sigmoid(gate) * product[:, half:]).astype(BF16)
    for k in range(members):
        out_ref[k] = hidden


def last_product(hidden_ref, down_ref, out_ref):
    total = dot(hidden_ref[0], down_ref[0])
    for k in range(1, hidden_ref.shape[0]):
        total = total + dot(hidden_ref[k], down_ref[k])
    out_ref[...] = total.astype(BF16)


def body(
    tokens,
    conv_state,
    lru_state,
    mix_gain,
    input_weight,
    branch_weight,
    conv_taps,
    conv_bias,
    recur_weight,
    recur_bias,
    inject_weight,
    inject_bias,
    decay_param,
    output_weight,
    moe_gain,
    route_ids,
    route_logits,
    group_weight,
    expert_gate,
    expert_up,
    expert_down,
):
    seq_count, quarter = tokens.shape
    members = lax.axis_size("tp")
    experts = lax.axis_size("ep")
    member = lax.axis_index("tp")
    place = member.astype(jnp.int32)[None]
    slots = experts * CAPACITY
    units = expert_gate.shape[2]

    token_parts = lax.all_to_all(
        jnp.broadcast_to(tokens[None], (members, *tokens.shape)), "tp", 0, 0, tiled=True
    )
    anywhere = pl.BlockSpec(memory_space=pl.ANY)
    pieces = pl.pallas_call(
        cut_weights,
        out_shape=[pltpu.VMEM((quarter // 2 + units, quarter), BF16)] * members,
        in_specs=[SMEM] + [anywhere] * 3,
        out_specs=[VMEM] * members,
        scratch_shapes=[pltpu.SemaphoreType.DMA((members, 5))],
    )(place, expert_gate, expert_up, expert_down)
    table = pltpu.VMEM((seq_count, slots), BF16)
    dispatch = call(dispatch_table, table, route_ids)
    combine_high, combine_low = call(
        combine_tables, [table] * 2, route_ids, route_logits, group_weight[:, None]
    )
    wide = token_parts.astype(F32)
    scale = lax.rsqrt(jnp.sum(wide * wide, axis=(0, 2)) / (members * quarter) + EPS)
    normed = (wide * scale[None, :, None] * mix_gain.reshape(members, 1, quarter)).astype(BF16)
    normed = side_by_side(normed)
    branch_x = dot(normed, input_weight).astype(BF16)
    branch_g = dot(normed, branch_weight).astype(BF16)
    window = jnp.concatenate([conv_state, branch_x[:, None, :]], axis=1)
    conv_sum = conv_bias + jnp.sum(window.astype(F32) * conv_taps[None], axis=1)
    conv_out = conv_sum.astype(BF16)
    recur_gate = block_gate(conv_out, recur_weight, recur_bias)
    inject_gate = block_gate(conv_out, inject_weight, inject_bias)
    log_rate = -RATE * recur_gate * jax.nn.softplus(-decay_param)
    new_state = jnp.exp(log_rate) * lru_state + jnp.sqrt(
        -jnp.expm1(2.0 * log_rate)
    ) * inject_gate * conv_out.astype(F32)
    mixer_out = (new_state * jax.nn.gelu(branch_g.astype(F32))).astype(BF16)
    copies = jnp.broadcast_to(mixer_out[None], (members, *mixer_out.shape))
    gain_part = lax.dynamic_slice_in_dim(moe_gain, member * quarter, quarter, 0)[None]
    copies, *sends = lax.optimization_barrier((copies, *pieces[1:]))
    mixer_parts = lax.all_to_all(copies, "tp", 0, 0, tiled=True)
    weights = [pieces[0]]
    for k in range(1, members):
        ring = [(m, (m + k) % members) for m in range(members)]
        weights.append(lax.ppermute(sends[k - 1], "tp", ring))
    stream = (tokens.astype(F32) + dot(side_by_side(mixer_parts), output_weight)).astype(BF16)

    outgoing = dot_on(dispatch, stream, 0, 0).astype(BF16).reshape(experts, CAPACITY, quarter)
    arrived = lax.all_to_all(outgoing, "ep", 0, 0, tiled=True)
    arrived = arrived.reshape(slots, quarter)
    products, down = call(
        first_products,
        [
            pltpu.VMEM((members, slots + SUM_ROWS, 2 * units), BF16),
            pltpu.VMEM((members, units, quarter), BF16),
        ],
        near(arrived),
        gain_part,
        near(jnp.stack(weights)),
        scalar=place,
    )
    products = lax.all_to_all(products, "tp", 0, 0, tiled=True)
    hidden = call(hidden_units, pltpu.VMEM((members, slots, units), BF16), near(products))
    hidden = lax.all_to_all(hidden, "tp", 0, 0, tiled=True)
    answer = call(
        last_product, pltpu.VMEM((slots, quarter), BF16), near(hidden), near(down)
    )
    returned = lax.all_to_all(answer, "ep", 0, 0, tiled=True)
    routed = dot(combine_high, returned) + dot(combine_low, returned)
    result = (stream.astype(F32) + routed).astype(BF16)
    return (result, new_state, window[:, 1:])


def solution(mesh):
    in_specs = (
        P("ep", "tp"),
        P("ep", None, "tp"),
        P("ep", "tp"),
        P(),
        P(None, "tp"),
        P(None, "tp"),
        P(None, "tp"),
        P("tp"),
        P("tp", None, None),
        P("tp"),
        P("tp", None, None),
        P("tp"),
        P("tp"),
        P(None, "tp"),
        P(),
        P("ep", None),
        P("ep", None),
        P("ep"),
        P("ep", None, "tp"),
        P("ep", None, "tp"),
        P("ep", "tp", None),
    )
    out_specs = (P("ep", "tp"), P("ep", "tp"), P("ep", None, "tp"))
    return jax.shard_map(body, mesh=mesh, in_specs=in_specs, out_specs=out_specs, check_vma=False)
```

```python
import functools

import jax
import jax.numpy as jnp
from jax import lax
from jax.experimental import pallas as pl
from jax.experimental.pallas import tpu as pltpu
from jax.sharding import PartitionSpec as P

EPS = 1e-06
RATE = 8.0
CAPACITY = 2
SUM_ROWS = 16
F32 = jnp.float32
BF16 = jnp.bfloat16
VMEM = pl.BlockSpec(memory_space=pltpu.VMEM)
SMEM = pl.BlockSpec(memory_space=pltpu.SMEM)


def near(value):
    return pltpu.with_memory_space_constraint(value, pltpu.VMEM)


def call(kernel, outs, *args, scalar=None):
    scalars = () if scalar is None else (scalar,)
    return pl.pallas_call(
        kernel,
        out_shape=outs,
        in_specs=[SMEM] * len(scalars) + [VMEM] * len(args),
        out_specs=jax.tree.map(lambda _: VMEM, outs),
    )(*scalars, *args)


def dot(a, b):
    return jnp.dot(a, b, preferred_element_type=F32)


def dot_on(a, b, a_dim, b_dim):
    return lax.dot_general(a, b, (((a_dim,), (b_dim,)), ((), ())), preferred_element_type=F32)


def halves(value):
    high = value.astype(BF16)
    return high, (value - high.astype(F32)).astype(BF16)


def places(ids_ref, count, slots):
    ids = ids_ref[...]
    column = lax.broadcasted_iota(jnp.int32, (count, slots), 1)
    expert = lax.div(column, CAPACITY)
    place = lax.rem(column, CAPACITY)
    first = ids[:, 0:1] == expert
    second = ids[:, 1:2] == expert
    named = jnp.where(first | second, 1.0, 0.0)
    below = lax.broadcasted_iota(jnp.int32, (count, count), 1) < lax.broadcasted_iota(
        jnp.int32, (count, count), 0
    )
    earlier = dot(jnp.where(below, 1.0, 0.0).astype(BF16), named.astype(BF16))
    return jnp.where(earlier == place.astype(F32), named, 0.0), first


def combine_tables(ids_ref, logits_ref, group_ref, piece_ref, high_ref, low_ref, near_ref, done):
    copy = pltpu.make_async_copy(piece_ref, near_ref, done)
    copy.start()
    hit, first = places(ids_ref, *high_ref.shape)
    raised = jnp.exp(logits_ref[...])
    weight = group_ref[...] * raised / (raised[:, 0:1] + raised[:, 1:2])
    high, low = halves(hit * jnp.where(first, weight[:, 0:1], weight[:, 1:2]))
    high_ref[...] = high
    low_ref[...] = low
    copy.wait()


def cut_weights(member_ref, gate_ref, up_ref, down_ref, *refs, members):
    *rest, piece_ref, reads, writes, loads = refs
    count = (len(rest) - members) // 2
    far_refs, out_refs, near_refs = rest[:count], rest[count : count + members], rest[count + members :]
    quarter = gate_ref.shape[1] // members
    half = quarter // 2
    width = gate_ref.shape[2]
    order = (2, 1, 3, 0)
    copies = {}
    for k in order:
        target = lax.rem(member_ref[0] + k, members)
        top = pl.multiple_of(target * quarter, quarter)
        piece = piece_ref.at[k]
        pairs = [(down_ref.at[0, :, pl.ds(top, quarter)], piece.at[pl.ds(half, width), :])]
        for part in range(2):
            rows = pl.ds(pl.multiple_of(top + part * half, half), half)
            at = part * 2 * width
            into = [piece.at[pl.ds(0, half), pl.ds(at + j * width, width)] for j in range(2)]
            pairs += [(gate_ref.at[0, rows, :], into[0]), (up_ref.at[0, rows, :], into[1])]
        copies[k] = [
            pltpu.make_async_copy(source, into, reads.at[k, j])
            for j, (source, into) in enumerate(pairs)
        ]
        for copy in copies[k]:
            copy.start()
    near_copies = [
        pltpu.make_async_copy(source, into, loads.at[j])
        for j, (source, into) in enumerate(zip(far_refs, near_refs))
    ]
    for copy in near_copies:
        copy.start()
    out_copies = []
    for k in order:
        for copy in copies[k]:
            copy.wait()
        out_copies.append(pltpu.make_async_copy(piece_ref.at[k], out_refs[k], writes.at[k]))
        out_copies[-1].start()
    for copy in near_copies + out_copies:
        copy.wait()


def mixer(
    parts_ref,
    gain_ref,
    input_ref,
    branch_ref,
    conv_ref,
    taps_ref,
    bias_ref,
    recur_ref,
    recur_bias_ref,
    inject_ref,
    inject_bias_ref,
    decay_ref,
    lru_ref,
    copies_ref,
    state_ref,
    window_ref,
):
    members, count, quarter = parts_ref.shape
    taps = taps_ref.shape[0]
    squares = jnp.zeros((count, 1), F32)
    for m in range(members):
        wide = parts_ref[m].astype(F32)
        squares = squares + jnp.sum(wide * wide, axis=1, keepdims=True)
    scale = lax.rsqrt(squares / (members * quarter) + EPS)
    normed = jnp.concatenate(
        [
            (
                parts_ref[m].astype(F32) * scale * gain_ref[:, m * quarter : (m + 1) * quarter]
            ).astype(BF16)
            for m in range(members)
        ],
        axis=1,
    )
    branch_x = dot(normed, input_ref[...]).astype(BF16)
    branch_g = dot(normed, branch_ref[...]).astype(BF16)
    rows = [conv_ref[j] for j in range(taps - 1)] + [branch_x]
    conv_sum = rows[0].astype(F32) * taps_ref[0:1]
    for j in range(1, taps):
        conv_sum = conv_sum + rows[j].astype(F32) * taps_ref[j : j + 1]
        window_ref[j - 1] = rows[j]
    conv_out = (bias_ref[...] + conv_sum).astype(BF16)
    blocks, size, _ = recur_ref.shape

    def gate(weight_ref, gate_bias_ref):
        product = [
            dot(conv_out[:, b * size : (b + 1) * size], weight_ref[b]) for b in range(blocks)
        ]
        return jax.nn.sigmoid(jnp.concatenate(product, axis=1) + gate_bias_ref[...])

    rate = -RATE * jax.nn.softplus(-decay_ref[...])
    log_rate = gate(recur_ref, recur_bias_ref) * rate
    inject = gate(inject_ref, inject_bias_ref)
    kept = jnp.exp(log_rate)
    rest = -jnp.tanh(log_rate) * (1.0 + kept * kept)
    state = kept * lru_ref[...] + jnp.sqrt(rest) * inject * conv_out.astype(F32)
    state_ref[...] = state
    out = (state * jax.nn.gelu(branch_g.astype(F32))).astype(BF16)
    for m in range(members):
        copies_ref[m] = out


def stream_rows(parts_ref, tokens_ref, ids_ref, weight_ref, stream_ref, out_ref, near_ref, done):
    copy = pltpu.make_async_copy(weight_ref, near_ref, done)
    copy.start()
    slots, count = out_ref.shape[0], tokens_ref.shape[0]
    row = lax.broadcasted_iota(jnp.int32, (slots, count), 0)
    expert = lax.div(row, CAPACITY)
    place = lax.rem(row, CAPACITY)
    ids = ids_ref[...]
    named = jnp.where((ids[0:1] == expert) | (ids[1:2] == expert), 1.0, 0.0)
    before = lax.broadcasted_iota(jnp.int32, (count, count), 0) < lax.broadcasted_iota(
        jnp.int32, (count, count), 1
    )
    earlier = dot(named.astype(BF16), jnp.where(before, 1.0, 0.0).astype(BF16))
    dispatch = jnp.where(earlier == place.astype(F32), named, 0.0).astype(BF16)
    copy.wait()
    members, _, width = parts_ref.shape
    mixed = dot(parts_ref[0], near_ref[:width, :])
    for m in range(1, members):
        mixed = mixed + dot(parts_ref[m], near_ref[m * width : (m + 1) * width, :])
    stream = (tokens_ref[...].astype(F32) + mixed).astype(BF16)
    stream_ref[...] = stream
    out_ref[...] = dot(dispatch, stream).astype(BF16)


def first_products(member_ref, rows_ref, gain_ref, *refs):
    *weight_refs, out_ref, down_ref = refs
    members = len(weight_refs)
    count, width = rows_ref.shape
    half = width // 2
    owners = [lax.rem(member_ref[0] + (members - k), members) for k in range(members)]
    rows = rows_ref[...].astype(F32)
    scaled = (rows * gain_ref[...]).astype(BF16)
    squares = rows * rows
    high, low = halves(squares)
    ones = jnp.ones((SUM_ROWS, width), BF16)
    sums_high, sums_low = halves(dot_on(ones, high, 1, 1) + dot_on(ones, low, 1, 1))
    place = lax.broadcasted_iota(jnp.int32, (SUM_ROWS, count), 0)
    sums = jnp.where(
        place == 0, sums_high.astype(F32), jnp.where(place == 1, sums_low.astype(F32), 0.0)
    ).astype(BF16)
    for k in range(members):
        out_ref[k, count:, :] = sums
    for k, cut in enumerate(weight_refs):
        down_ref[owners[k]] = cut[half:, :]
        product = dot(scaled[:, :half], cut[:half, :half]) + dot(
            scaled[:, half:], cut[:half, half:]
        )
        out_ref[owners[k], :count, :] = product.astype(BF16)


def hidden_units(parts_ref, out_ref):
    members, total, width = parts_ref.shape
    count = total - SUM_ROWS
    half = width // 2
    product = parts_ref[0, :count, :].astype(F32)
    sums = parts_ref[0, count:, :].astype(F32)
    for k in range(1, members):
        product = product + parts_ref[k, :count, :].astype(F32)
        sums = sums + parts_ref[k, count:, :].astype(F32)
    row_sum = jnp.sum(jnp.transpose(sums), axis=1, keepdims=True)
    product = product * lax.rsqrt(row_sum / (members * 2 * width) + EPS)
    gate = product[:, :half]
    hidden = (gate * jax.nn.sigmoid(gate) * product[:, half:]).astype(BF16)
    for k in range(members):
        out_ref[k] = hidden


def last_product(hidden_ref, down_ref, out_ref):
    total = dot(hidden_ref[0], down_ref[0])
    for k in range(1, hidden_ref.shape[0]):
        total = total + dot(hidden_ref[k], down_ref[k])
    out_ref[...] = total.astype(BF16)


def body(
    tokens,
    conv_state,
    lru_state,
    mix_gain,
    input_weight,
    branch_weight,
    conv_taps,
    conv_bias,
    recur_weight,
    recur_bias,
    inject_weight,
    inject_bias,
    decay_param,
    output_weight,
    moe_gain,
    route_ids,
    route_logits,
    group_weight,
    expert_gate,
    expert_up,
    expert_down,
):
    seq_count, quarter = tokens.shape
    channels = lru_state.shape[1]
    members = lax.axis_size("tp")
    experts = lax.axis_size("ep")
    member = lax.axis_index("tp")
    place = member.astype(jnp.int32)[None]
    slots = experts * CAPACITY
    units = expert_gate.shape[2]

    token_parts = lax.all_to_all(
        jnp.broadcast_to(tokens[None], (members, *tokens.shape)), "tp", 0, 0, tiled=True
    )
    anywhere = pl.BlockSpec(memory_space=pl.ANY)
    piece = (quarter // 2 + units, quarter)
    operands = [
        mix_gain[None],
        input_weight,
        branch_weight,
        jnp.swapaxes(conv_state, 0, 1),
        conv_taps,
        conv_bias[None],
        recur_weight,
        recur_bias[None],
        inject_weight,
        inject_bias[None],
        decay_param[None],
        lru_state,
    ]
    cutting = pl.pallas_call(
        functools.partial(cut_weights, members=members),
        out_shape=[jax.ShapeDtypeStruct(piece, BF16)] * members
        + [pltpu.VMEM(value.shape, value.dtype) for value in operands],
        in_specs=[SMEM] + [anywhere] * (3 + len(operands)),
        out_specs=[anywhere] * members + [VMEM] * len(operands),
        scratch_shapes=[
            pltpu.VMEM((members, *piece), BF16),
            pltpu.SemaphoreType.DMA((members, 5)),
            pltpu.SemaphoreType.DMA((members,)),
            pltpu.SemaphoreType.DMA((len(operands),)),
        ],
    )
    loaded = cutting(place, expert_gate, expert_up, expert_down, *operands)
    pieces, operands = loaded[:members], loaded[members:]
    table = pltpu.VMEM((seq_count, slots), BF16)
    combine_high, combine_low, own_piece = pl.pallas_call(
        combine_tables,
        out_shape=[table, table, pltpu.VMEM(piece, BF16)],
        in_specs=[VMEM] * 3 + [anywhere],
        out_specs=[VMEM] * 3,
        scratch_shapes=[pltpu.SemaphoreType.DMA],
    )(route_ids, route_logits, group_weight[:, None], pieces[0])
    copies, new_state, window = call(
        mixer,
        [
            pltpu.VMEM((members, seq_count, channels), BF16),
            jax.ShapeDtypeStruct((seq_count, channels), F32),
            jax.ShapeDtypeStruct((conv_state.shape[1], seq_count, channels), BF16),
        ],
        near(token_parts),
        *[near(value) for value in operands],
    )
    first_feature = member * quarter
    gain_part = lax.dynamic_slice_in_dim(moe_gain, first_feature, quarter, 0)[None]
    mixer_parts = lax.all_to_all(copies, "tp", 0, 0, tiled=True)
    weights = []
    for k in range(1, members):
        ring = [(m, (m + k) % members) for m in range(members)]
        weights.append(lax.ppermute(pieces[k], "tp", ring))
    stream, outgoing = pl.pallas_call(
        stream_rows,
        out_shape=[pltpu.VMEM((seq_count, quarter), BF16), pltpu.VMEM((slots, quarter), BF16)],
        in_specs=[VMEM] * 3 + [anywhere],
        out_specs=[VMEM] * 2,
        scratch_shapes=[pltpu.VMEM(output_weight.shape, BF16), pltpu.SemaphoreType.DMA],
    )(near(mixer_parts), tokens, route_ids.T, output_weight)

    outgoing = outgoing.reshape(experts, CAPACITY, quarter)
    arrived = lax.all_to_all(outgoing, "ep", 0, 0, tiled=True)
    arrived = arrived.reshape(slots, quarter)
    products, down = call(
        first_products,
        [
            pltpu.VMEM((members, slots + SUM_ROWS, 2 * units), BF16),
            pltpu.VMEM((members, units, quarter), BF16),
        ],
        near(arrived),
        gain_part,
        near(own_piece),
        *[near(w) for w in weights],
        scalar=place,
    )
    products = lax.all_to_all(products, "tp", 0, 0, tiled=True)
    hidden = call(hidden_units, pltpu.VMEM((members, slots, units), BF16), near(products))
    hidden = lax.all_to_all(hidden, "tp", 0, 0, tiled=True)
    answer = call(
        last_product, pltpu.VMEM((slots, quarter), BF16), near(hidden), near(down)
    )
    returned = lax.all_to_all(answer, "ep", 0, 0, tiled=True)
    routed = dot(combine_high, returned) + dot(combine_low, returned)
    result = (stream.astype(F32) + routed).astype(BF16)
    return (result, new_state, jnp.swapaxes(window, 0, 1))


def solution(mesh):
    in_specs = (
        P("ep", "tp"),
        P("ep", None, "tp"),
        P("ep", "tp"),
        P(),
        P(None, "tp"),
        P(None, "tp"),
        P(None, "tp"),
        P("tp"),
        P("tp", None, None),
        P("tp"),
        P("tp", None, None),
        P("tp"),
        P("tp"),
        P(None, "tp"),
        P(),
        P("ep", None),
        P("ep", None),
        P("ep"),
        P("ep", None, "tp"),
        P("ep", None, "tp"),
        P("ep", "tp", None),
    )
    out_specs = (P("ep", "tp"), P("ep", "tp"), P("ep", None, "tp"))
    return jax.shard_map(body, mesh=mesh, in_specs=in_specs, out_specs=out_specs, check_vma=False)
```

```python
import functools

import jax
import jax.numpy as jnp
from jax import lax
from jax.experimental import pallas as pl
from jax.experimental.pallas import tpu as pltpu
from jax.sharding import PartitionSpec as P

EPS = 1e-06
RATE = 8.0
CAPACITY = 2
SUM_ROWS = 16
F32 = jnp.float32
BF16 = jnp.bfloat16
VMEM = pl.BlockSpec(memory_space=pltpu.VMEM)
SMEM = pl.BlockSpec(memory_space=pltpu.SMEM)


def near(value):
    return pltpu.with_memory_space_constraint(value, pltpu.VMEM)


def call(kernel, outs, *args, scalar=None):
    scalars = () if scalar is None else (scalar,)
    return pl.pallas_call(
        kernel,
        out_shape=outs,
        in_specs=[SMEM] * len(scalars) + [VMEM] * len(args),
        out_specs=jax.tree.map(lambda _: VMEM, outs),
    )(*scalars, *args)


def dot(a, b):
    return jnp.dot(a, b, preferred_element_type=F32)


def dot_on(a, b, a_dim, b_dim):
    return lax.dot_general(a, b, (((a_dim,), (b_dim,)), ((), ())), preferred_element_type=F32)


def halves(value):
    high = value.astype(BF16)
    return high, (value - high.astype(F32)).astype(BF16)


def places(ids_ref, slots):
    ids = ids_ref[...]
    count = ids.shape[1]
    row = lax.broadcasted_iota(jnp.int32, (slots, count), 0)
    expert = lax.div(row, CAPACITY)
    place = lax.rem(row, CAPACITY)
    first = ids[0:1] == expert
    named = jnp.where(first | (ids[1:2] == expert), 1.0, 0.0)
    before = lax.broadcasted_iota(jnp.int32, (count, count), 0) < lax.broadcasted_iota(
        jnp.int32, (count, count), 1
    )
    earlier = dot(named.astype(BF16), jnp.where(before, 1.0, 0.0).astype(BF16))
    return jnp.where(earlier == place.astype(F32), named, 0.0), first


def dispatch_table(
    ids_ref, weight_ref, tokens_ref, out_ref, weight_near_ref, tokens_near_ref, ids_near_ref, done
):
    copies = [
        pltpu.make_async_copy(source, into, done.at[j])
        for j, (source, into) in enumerate(
            [
                (ids_ref, ids_near_ref),
                (weight_ref, weight_near_ref),
                (tokens_ref, tokens_near_ref),
            ]
        )
    ]
    for copy in copies:
        copy.start()
    copies[0].wait()
    out_ref[...] = places(ids_near_ref, out_ref.shape[0])[0].astype(BF16)
    for copy in copies[1:]:
        copy.wait()


def combine_tables(
    member_ref,
    ids_ref,
    logits_ref,
    group_ref,
    piece_ref,
    gain_ref,
    high_ref,
    low_ref,
    piece_near_ref,
    gain_near_ref,
    done,
):
    quarter = gain_near_ref.shape[1]
    own = pl.multiple_of(member_ref[0] * quarter, quarter)
    copies = [
        pltpu.make_async_copy(piece_ref, piece_near_ref, done.at[0]),
        pltpu.make_async_copy(gain_ref.at[:, pl.ds(own, quarter)], gain_near_ref, done.at[1]),
    ]
    for copy in copies:
        copy.start()
    hit, first = places(ids_ref, high_ref.shape[0])
    raised = jnp.exp(logits_ref[...])
    weight = group_ref[...] * raised / (raised[0:1] + raised[1:2])
    high, low = halves(hit * jnp.where(first, weight[0:1], weight[1:2]))
    high_ref[...] = high
    low_ref[...] = low
    for copy in copies:
        copy.wait()


def cut_weights(member_ref, gate_ref, up_ref, down_ref, *refs, members):
    *rest, piece_ref, reads, writes, loads = refs
    pieces = 2 * members - 2
    count = (len(rest) - pieces) // 2
    far_refs, rest = rest[:count], rest[count:]
    out_refs, near_refs = rest[:pieces], rest[pieces:]
    quarter = gate_ref.shape[1] // members
    half = quarter // 2
    width = gate_ref.shape[2]
    order = (2, 1, 3, 0)
    copies = {}
    for k in order:
        target = lax.rem(member_ref[0] + k, members)
        top = pl.multiple_of(target * quarter, quarter)
        piece = piece_ref.at[k]
        pairs = [(down_ref.at[0, :, pl.ds(top, quarter)], piece.at[pl.ds(half, width), :])]
        for part in range(2):
            rows = pl.ds(pl.multiple_of(top + part * half, half), half)
            at = part * 2 * width
            into = [piece.at[pl.ds(0, half), pl.ds(at + j * width, width)] for j in range(2)]
            pairs += [(gate_ref.at[0, rows, :], into[0]), (up_ref.at[0, rows, :], into[1])]
        copies[k] = [
            pltpu.make_async_copy(source, into, reads.at[k, j])
            for j, (source, into) in enumerate(pairs)
        ]
        for copy in copies[k]:
            copy.start()
    near_copies = [
        pltpu.make_async_copy(source, into, loads.at[j])
        for j, (source, into) in enumerate(zip(far_refs, near_refs))
    ]
    for copy in near_copies:
        copy.start()
    whole = pl.ds(0, half + width)
    parts = [(0, whole), (2, whole)]
    for k in (1, 3):
        parts += [(k, pl.ds(0, half)), (k, pl.ds(half, width))]
    out_copies = []
    for k in order:
        for copy in copies[k]:
            copy.wait()
        for j, (owner, rows) in enumerate(parts):
            if owner == k:
                copy = pltpu.make_async_copy(piece_ref.at[k, rows], out_refs[j], writes.at[j])
                copy.start()
                out_copies.append(copy)
    for copy in near_copies + out_copies:
        copy.wait()


def mixer(
    parts_ref,
    gain_ref,
    input_ref,
    branch_ref,
    conv_ref,
    taps_ref,
    bias_ref,
    recur_ref,
    recur_bias_ref,
    inject_ref,
    inject_bias_ref,
    decay_ref,
    lru_ref,
    copies_ref,
    state_ref,
    window_ref,
):
    members, count, quarter = parts_ref.shape
    taps = taps_ref.shape[0]
    squares = jnp.zeros((count, 1), F32)
    for m in range(members):
        wide = parts_ref[m].astype(F32)
        squares = squares + jnp.sum(wide * wide, axis=1, keepdims=True)
    scale = lax.rsqrt(squares / (members * quarter) + EPS)
    normed = jnp.concatenate(
        [
            (
                parts_ref[m].astype(F32) * scale * gain_ref[:, m * quarter : (m + 1) * quarter]
            ).astype(BF16)
            for m in range(members)
        ],
        axis=1,
    )
    branch_x = dot(normed, input_ref[...]).astype(BF16)
    branch_g = dot(normed, branch_ref[...]).astype(BF16)
    rows = [conv_ref[j] for j in range(taps - 1)] + [branch_x]
    conv_sum = rows[0].astype(F32) * taps_ref[0:1]
    for j in range(1, taps):
        conv_sum = conv_sum + rows[j].astype(F32) * taps_ref[j : j + 1]
        window_ref[j - 1] = rows[j]
    conv_out = (bias_ref[...] + conv_sum).astype(BF16)
    blocks, size, _ = recur_ref.shape

    def gate(weight_ref, gate_bias_ref):
        product = [
            dot(conv_out[:, b * size : (b + 1) * size], weight_ref[b]) for b in range(blocks)
        ]
        return jax.nn.sigmoid(jnp.concatenate(product, axis=1) + gate_bias_ref[...])

    rate = -RATE * jax.nn.softplus(-decay_ref[...])
    log_rate = gate(recur_ref, recur_bias_ref) * rate
    inject = gate(inject_ref, inject_bias_ref)
    kept = jnp.exp(log_rate)
    rest = -jnp.tanh(log_rate) * (1.0 + kept * kept)
    state = kept * lru_ref[...] + jnp.sqrt(rest) * inject * conv_out.astype(F32)
    state_ref[...] = state
    out = (state * jax.nn.gelu(branch_g.astype(F32))).astype(BF16)
    for m in range(members):
        copies_ref[m] = out


def stream_rows(parts_ref, weight_ref, tokens_ref, dispatch_ref, stream_ref, out_ref):
    members, _, width = parts_ref.shape
    mixed = dot(parts_ref[0], weight_ref[:width, :])
    for m in range(1, members):
        mixed = mixed + dot(parts_ref[m], weight_ref[m * width : (m + 1) * width, :])
    stream = (tokens_ref[...].astype(F32) + mixed).astype(BF16)
    stream_ref[...] = stream
    out_ref[...] = dot(dispatch_ref[...], stream).astype(BF16)


def first_products(member_ref, rows_ref, gain_ref, *refs):
    *weight_refs, out_ref = refs
    members = len(weight_refs)
    count, width = rows_ref.shape
    half = width // 2
    owners = [lax.rem(member_ref[0] + (members - k), members) for k in range(members)]
    rows = rows_ref[...].astype(F32)
    scaled = (rows * gain_ref[...]).astype(BF16)
    squares = rows * rows
    high, low = halves(squares)
    ones = jnp.ones((SUM_ROWS, width), BF16)
    sums_high, sums_low = halves(dot_on(ones, high, 1, 1) + dot_on(ones, low, 1, 1))
    place = lax.broadcasted_iota(jnp.int32, (SUM_ROWS, count), 0)
    sums = jnp.where(
        place == 0, sums_high.astype(F32), jnp.where(place == 1, sums_low.astype(F32), 0.0)
    ).astype(BF16)
    for k in range(members):
        out_ref[k, count:, :] = sums
    for k, cut in enumerate(weight_refs):
        product = dot(scaled[:, :half], cut[:half, :half]) + dot(
            scaled[:, half:], cut[:half, half:]
        )
        out_ref[owners[k], :count, :] = product.astype(BF16)


def hidden_units(parts_ref, out_ref):
    members, total, width = parts_ref.shape
    count = total - SUM_ROWS
    half = width // 2
    product = parts_ref[0, :count, :].astype(F32)
    sums = parts_ref[0, count:, :].astype(F32)
    for k in range(1, members):
        product = product + parts_ref[k, :count, :].astype(F32)
        sums = sums + parts_ref[k, count:, :].astype(F32)
    row_sum = jnp.sum(jnp.transpose(sums), axis=1, keepdims=True)
    product = product * lax.rsqrt(row_sum / (members * 2 * width) + EPS)
    gate = product[:, :half]
    hidden = (gate * jax.nn.sigmoid(gate) * product[:, half:]).astype(BF16)
    for k in range(members):
        out_ref[k] = hidden


def last_product(member_ref, hidden_ref, *refs):
    *weight_refs, out_ref = refs
    members, _, width = hidden_ref.shape
    total = jnp.zeros(out_ref.shape, F32)
    for k, weight_ref in enumerate(weight_refs):
        owner = lax.rem(member_ref[0] + (members - k), members)
        total = total + dot(hidden_ref[owner], weight_ref[weight_ref.shape[0] - width :, :])
    out_ref[...] = total.astype(BF16)


def body(
    tokens,
    conv_state,
    lru_state,
    mix_gain,
    input_weight,
    branch_weight,
    conv_taps,
    conv_bias,
    recur_weight,
    recur_bias,
    inject_weight,
    inject_bias,
    decay_param,
    output_weight,
    moe_gain,
    route_ids,
    route_logits,
    group_weight,
    expert_gate,
    expert_up,
    expert_down,
):
    seq_count, quarter = tokens.shape
    channels = lru_state.shape[1]
    members = lax.axis_size("tp")
    experts = lax.axis_size("ep")
    member = lax.axis_index("tp")
    place = member.astype(jnp.int32)[None]
    slots = experts * CAPACITY
    units = expert_gate.shape[2]

    token_parts = lax.all_to_all(
        jnp.broadcast_to(tokens[None], (members, *tokens.shape)), "tp", 0, 0, tiled=True
    )
    anywhere = pl.BlockSpec(memory_space=pl.ANY)
    operands = [
        mix_gain[None],
        input_weight,
        branch_weight,
        jnp.swapaxes(conv_state, 0, 1),
        conv_taps,
        conv_bias[None],
        recur_weight,
        recur_bias[None],
        inject_weight,
        inject_bias[None],
        decay_param[None],
        lru_state,
    ]
    half, whole = (quarter // 2, quarter), (quarter // 2 + units, quarter)
    cuts = [whole, whole, half, (units, quarter), half, (units, quarter)]
    cutting = pl.pallas_call(
        functools.partial(cut_weights, members=members),
        out_shape=[jax.ShapeDtypeStruct(shape, BF16) for shape in cuts]
        + [pltpu.VMEM(value.shape, value.dtype) for value in operands],
        in_specs=[SMEM] + [anywhere] * (3 + len(operands)),
        out_specs=[anywhere] * len(cuts) + [VMEM] * len(operands),
        scratch_shapes=[
            pltpu.VMEM((members, *whole), BF16),
            pltpu.SemaphoreType.DMA((members, 5)),
            pltpu.SemaphoreType.DMA((len(cuts),)),
            pltpu.SemaphoreType.DMA((len(operands),)),
        ],
    )
    loaded = cutting(place, expert_gate, expert_up, expert_down, *operands)
    own, across, *sides = loaded[: len(cuts)]
    operands = [near(value) for value in loaded[len(cuts) :]]
    table = pltpu.VMEM((slots, seq_count), BF16)
    ids = route_ids.T
    dispatch, output_near, tokens_near = pl.pallas_call(
        dispatch_table,
        out_shape=[table, pltpu.VMEM(output_weight.shape, BF16), pltpu.VMEM(tokens.shape, BF16)],
        in_specs=[anywhere] * 3,
        out_specs=[VMEM] * 3,
        scratch_shapes=[
            pltpu.VMEM(ids.shape, ids.dtype),
            pltpu.SemaphoreType.DMA((3,)),
        ],
    )(ids, output_weight, tokens)
    combine_high, combine_low, own, gain_part = pl.pallas_call(
        combine_tables,
        out_shape=[table, table, pltpu.VMEM(whole, BF16), pltpu.VMEM((1, quarter), F32)],
        in_specs=[SMEM] + [VMEM] * 3 + [anywhere] * 2,
        out_specs=[VMEM] * 4,
        scratch_shapes=[pltpu.SemaphoreType.DMA((2,))],
    )(place, ids, route_logits.T, group_weight[None], own, moe_gain[None])
    copies, new_state, window = call(
        mixer,
        [
            pltpu.VMEM((members, seq_count, channels), BF16),
            jax.ShapeDtypeStruct((seq_count, channels), F32),
            jax.ShapeDtypeStruct((conv_state.shape[1], seq_count, channels), BF16),
        ],
        near(token_parts),
        *operands,
    )
    mixer_parts = lax.all_to_all(copies, "tp", 0, 0, tiled=True)

    def onward(value, step):
        ring = [(m, (m + step) % members) for m in range(members)]
        return lax.ppermute(value, "tp", ring)

    across = onward(across, 2)
    cut_next = onward(sides[0], 1)
    cut_last = onward(sides[2], 3)
    down_next = onward(sides[1], 1)
    down_last = onward(sides[3], 3)
    stream, outgoing = call(
        stream_rows,
        [pltpu.VMEM((seq_count, quarter), BF16), pltpu.VMEM((slots, quarter), BF16)],
        near(mixer_parts),
        near(output_near),
        near(tokens_near),
        near(dispatch),
    )

    outgoing = outgoing.reshape(experts, CAPACITY, quarter)
    arrived = lax.all_to_all(outgoing, "ep", 0, 0, tiled=True)
    arrived = arrived.reshape(slots, quarter)
    own, across = near(own), near(across)
    products = call(
        first_products,
        pltpu.VMEM((members, slots + SUM_ROWS, 2 * units), BF16),
        near(arrived),
        near(gain_part),
        own,
        near(cut_next),
        across,
        near(cut_last),
        scalar=place,
    )
    products = lax.all_to_all(products, "tp", 0, 0, tiled=True)
    hidden = call(hidden_units, pltpu.VMEM((members, slots, units), BF16), near(products))
    hidden, down_next, down_last = lax.optimization_barrier((hidden, down_next, down_last))
    hidden = lax.all_to_all(hidden, "tp", 0, 0, tiled=True)
    answer = call(
        last_product,
        pltpu.VMEM((slots, quarter), BF16),
        near(hidden),
        own,
        near(down_next),
        across,
        near(down_last),
        scalar=place,
    )
    returned = lax.all_to_all(answer, "ep", 0, 0, tiled=True)
    routed = dot_on(combine_high, returned, 0, 0) + dot_on(combine_low, returned, 0, 0)
    result = (stream.astype(F32) + routed).astype(BF16)
    return (result, new_state, jnp.swapaxes(window, 0, 1))


def solution(mesh):
    in_specs = (
        P("ep", "tp"),
        P("ep", None, "tp"),
        P("ep", "tp"),
        P(),
        P(None, "tp"),
        P(None, "tp"),
        P(None, "tp"),
        P("tp"),
        P("tp", None, None),
        P("tp"),
        P("tp", None, None),
        P("tp"),
        P("tp"),
        P(None, "tp"),
        P(),
        P("ep", None),
        P("ep", None),
        P("ep"),
        P("ep", None, "tp"),
        P("ep", None, "tp"),
        P("ep", "tp", None),
    )
    out_specs = (P("ep", "tp"), P("ep", "tp"), P("ep", None, "tp"))
    return jax.shard_map(body, mesh=mesh, in_specs=in_specs, out_specs=out_specs, check_vma=False)
```

```python
import functools

import jax
import jax.numpy as jnp
from jax import lax
from jax.experimental import pallas as pl
from jax.experimental.pallas import tpu as pltpu
from jax.sharding import PartitionSpec as P

EPS = 1e-06
RATE = 8.0
CAPACITY = 2
SUM_ROWS = 16
F32 = jnp.float32
BF16 = jnp.bfloat16
VMEM = pl.BlockSpec(memory_space=pltpu.VMEM)
SMEM = pl.BlockSpec(memory_space=pltpu.SMEM)


def near(value):
    return pltpu.with_memory_space_constraint(value, pltpu.VMEM)


def call(kernel, outs, *args, scalar=None):
    scalars = () if scalar is None else (scalar,)
    return pl.pallas_call(
        kernel,
        out_shape=outs,
        in_specs=[SMEM] * len(scalars) + [VMEM] * len(args),
        out_specs=jax.tree.map(lambda _: VMEM, outs),
    )(*scalars, *args)


def dot(a, b):
    return jnp.dot(a, b, preferred_element_type=F32)


def dot_on(a, b, a_dim, b_dim):
    return lax.dot_general(a, b, (((a_dim,), (b_dim,)), ((), ())), preferred_element_type=F32)


def halves(value):
    high = value.astype(BF16)
    return high, (value - high.astype(F32)).astype(BF16)


def places(ids_ref, slots):
    ids = ids_ref[...]
    count = ids.shape[1]
    row = lax.broadcasted_iota(jnp.int32, (slots, count), 0)
    expert = lax.div(row, CAPACITY)
    place = lax.rem(row, CAPACITY)
    first = ids[0:1] == expert
    named = jnp.where(first | (ids[1:2] == expert), 1.0, 0.0)
    before = lax.broadcasted_iota(jnp.int32, (count, count), 0) < lax.broadcasted_iota(
        jnp.int32, (count, count), 1
    )
    earlier = dot(named.astype(BF16), jnp.where(before, 1.0, 0.0).astype(BF16))
    return jnp.where(earlier == place.astype(F32), named, 0.0), first


def dispatch_table(
    member_ref,
    ids_ref,
    weight_ref,
    tokens_ref,
    gain_ref,
    out_ref,
    weight_near_ref,
    tokens_near_ref,
    gain_near_ref,
    ids_near_ref,
    done,
):
    quarter = gain_near_ref.shape[1]
    own = pl.multiple_of(member_ref[0] * quarter, quarter)
    pairs = [
        (ids_ref, ids_near_ref),
        (weight_ref, weight_near_ref),
        (tokens_ref, tokens_near_ref),
        (gain_ref.at[:, pl.ds(own, quarter)], gain_near_ref),
    ]
    copies = [
        pltpu.make_async_copy(source, into, done.at[j]) for j, (source, into) in enumerate(pairs)
    ]
    for copy in copies:
        copy.start()
    copies[0].wait()
    out_ref[...] = places(ids_near_ref, out_ref.shape[0])[0].astype(BF16)
    for copy in copies[1:]:
        copy.wait()


def combine_tables(ids_ref, logits_ref, group_ref, high_ref, low_ref):
    hit, first = places(ids_ref, high_ref.shape[0])
    raised = jnp.exp(logits_ref[...])
    weight = group_ref[...] * raised / (raised[0:1] + raised[1:2])
    high, low = halves(hit * jnp.where(first, weight[0:1], weight[1:2]))
    high_ref[...] = high
    low_ref[...] = low


def cut_weights(member_ref, gate_ref, up_ref, down_ref, *refs, members):
    *rest, piece_ref, reads, writes, loads = refs
    pieces = 2 * members - 2
    count = (len(rest) - pieces) // 2
    far_refs, rest = rest[:count], rest[count:]
    out_refs, near_refs = rest[:pieces], rest[pieces:]
    quarter = gate_ref.shape[1] // members
    half = quarter // 2
    width = gate_ref.shape[2]
    order = (2, 1, 3, 0)
    copies = {}
    for k in order:
        target = lax.rem(member_ref[0] + k, members)
        top = pl.multiple_of(target * quarter, quarter)
        piece = piece_ref.at[k]
        pairs = [(down_ref.at[0, :, pl.ds(top, quarter)], piece.at[pl.ds(half, width), :])]
        for part in range(2):
            rows = pl.ds(pl.multiple_of(top + part * half, half), half)
            at = part * 2 * width
            into = [piece.at[pl.ds(0, half), pl.ds(at + j * width, width)] for j in range(2)]
            pairs += [(gate_ref.at[0, rows, :], into[0]), (up_ref.at[0, rows, :], into[1])]
        copies[k] = [
            pltpu.make_async_copy(source, into, reads.at[k, j])
            for j, (source, into) in enumerate(pairs)
        ]
        for copy in copies[k]:
            copy.start()
    near_copies = [
        pltpu.make_async_copy(source, into, loads.at[j])
        for j, (source, into) in enumerate(zip(far_refs, near_refs))
    ]
    for copy in near_copies:
        copy.start()
    whole = pl.ds(0, half + width)
    parts = [(0, whole), (2, whole)]
    for k in (1, 3):
        parts += [(k, pl.ds(0, half)), (k, pl.ds(half, width))]
    out_copies = []
    for k in order:
        for copy in copies[k]:
            copy.wait()
        for j, (owner, rows) in enumerate(parts):
            if owner == k:
                copy = pltpu.make_async_copy(piece_ref.at[k, rows], out_refs[j], writes.at[j])
                copy.start()
                out_copies.append(copy)
    for copy in near_copies + out_copies:
        copy.wait()


def mixer(
    parts_ref,
    gain_ref,
    input_ref,
    branch_ref,
    conv_ref,
    taps_ref,
    bias_ref,
    recur_ref,
    recur_bias_ref,
    inject_ref,
    inject_bias_ref,
    decay_ref,
    lru_ref,
    copies_ref,
    state_ref,
    window_ref,
):
    members, count, quarter = parts_ref.shape
    taps = taps_ref.shape[0]
    squares = jnp.zeros((count, 1), F32)
    for m in range(members):
        wide = parts_ref[m].astype(F32)
        squares = squares + jnp.sum(wide * wide, axis=1, keepdims=True)
    scale = lax.rsqrt(squares / (members * quarter) + EPS)
    normed = jnp.concatenate(
        [
            (
                parts_ref[m].astype(F32) * scale * gain_ref[:, m * quarter : (m + 1) * quarter]
            ).astype(BF16)
            for m in range(members)
        ],
        axis=1,
    )
    branch_x = dot(normed, input_ref[...]).astype(BF16)
    branch_g = dot(normed, branch_ref[...]).astype(BF16)
    rows = [conv_ref[j] for j in range(taps - 1)] + [branch_x]
    conv_sum = rows[0].astype(F32) * taps_ref[0:1]
    for j in range(1, taps):
        conv_sum = conv_sum + rows[j].astype(F32) * taps_ref[j : j + 1]
        window_ref[j - 1] = rows[j]
    conv_out = (bias_ref[...] + conv_sum).astype(BF16)
    blocks, size, _ = recur_ref.shape

    def gate(weight_ref, gate_bias_ref):
        product = [
            dot(conv_out[:, b * size : (b + 1) * size], weight_ref[b]) for b in range(blocks)
        ]
        return jax.nn.sigmoid(jnp.concatenate(product, axis=1) + gate_bias_ref[...])

    rate = -RATE * jax.nn.softplus(-decay_ref[...])
    log_rate = gate(recur_ref, recur_bias_ref) * rate
    inject = gate(inject_ref, inject_bias_ref)
    kept = jnp.exp(log_rate)
    rest = -jnp.tanh(log_rate) * (1.0 + kept * kept)
    state = kept * lru_ref[...] + jnp.sqrt(rest) * inject * conv_out.astype(F32)
    state_ref[...] = state
    out = (state * jax.nn.gelu(branch_g.astype(F32))).astype(BF16)
    for m in range(members):
        copies_ref[m] = out


def stream_rows(parts_ref, weight_ref, tokens_ref, dispatch_ref, stream_ref, out_ref):
    members, _, width = parts_ref.shape
    mixed = dot(parts_ref[0], weight_ref[:width, :])
    for m in range(1, members):
        mixed = mixed + dot(parts_ref[m], weight_ref[m * width : (m + 1) * width, :])
    stream = (tokens_ref[...].astype(F32) + mixed).astype(BF16)
    stream_ref[...] = stream
    out_ref[...] = dot(dispatch_ref[...], stream).astype(BF16)


def first_products(member_ref, rows_ref, gain_ref, *refs):
    *weight_refs, out_ref = refs
    members = len(weight_refs)
    count, width = rows_ref.shape
    half = width // 2
    owners = [lax.rem(member_ref[0] + (members - k), members) for k in range(members)]
    rows = rows_ref[...].astype(F32)
    scaled = (rows * gain_ref[...]).astype(BF16)
    squares = rows * rows
    high, low = halves(squares)
    ones = jnp.ones((SUM_ROWS, width), BF16)
    sums_high, sums_low = halves(dot_on(ones, high, 1, 1) + dot_on(ones, low, 1, 1))
    place = lax.broadcasted_iota(jnp.int32, (SUM_ROWS, count), 0)
    sums = jnp.where(
        place == 0, sums_high.astype(F32), jnp.where(place == 1, sums_low.astype(F32), 0.0)
    ).astype(BF16)
    for k in range(members):
        out_ref[k, count:, :] = sums
    for k, cut in enumerate(weight_refs):
        product = dot(scaled[:, :half], cut[:half, :half]) + dot(
            scaled[:, half:], cut[:half, half:]
        )
        out_ref[owners[k], :count, :] = product.astype(BF16)


def hidden_units(parts_ref, out_ref):
    members, total, width = parts_ref.shape
    count = total - SUM_ROWS
    half = width // 2
    product = parts_ref[0, :count, :].astype(F32)
    sums = parts_ref[0, count:, :].astype(F32)
    for k in range(1, members):
        product = product + parts_ref[k, :count, :].astype(F32)
        sums = sums + parts_ref[k, count:, :].astype(F32)
    row_sum = jnp.sum(jnp.transpose(sums), axis=1, keepdims=True)
    product = product * lax.rsqrt(row_sum / (members * 2 * width) + EPS)
    gate = product[:, :half]
    hidden = (gate * jax.nn.sigmoid(gate) * product[:, half:]).astype(BF16)
    for k in range(members):
        out_ref[k] = hidden


def last_product(member_ref, hidden_ref, *refs):
    *weight_refs, out_ref = refs
    members, _, width = hidden_ref.shape
    total = jnp.zeros(out_ref.shape, F32)
    for k, weight_ref in enumerate(weight_refs):
        owner = lax.rem(member_ref[0] + (members - k), members)
        total = total + dot(hidden_ref[owner], weight_ref[weight_ref.shape[0] - width :, :])
    out_ref[...] = total.astype(BF16)


def body(
    tokens,
    conv_state,
    lru_state,
    mix_gain,
    input_weight,
    branch_weight,
    conv_taps,
    conv_bias,
    recur_weight,
    recur_bias,
    inject_weight,
    inject_bias,
    decay_param,
    output_weight,
    moe_gain,
    route_ids,
    route_logits,
    group_weight,
    expert_gate,
    expert_up,
    expert_down,
):
    seq_count, quarter = tokens.shape
    channels = lru_state.shape[1]
    members = lax.axis_size("tp")
    experts = lax.axis_size("ep")
    member = lax.axis_index("tp")
    place = member.astype(jnp.int32)[None]
    slots = experts * CAPACITY
    units = expert_gate.shape[2]

    token_parts = lax.all_to_all(
        jnp.broadcast_to(tokens[None], (members, *tokens.shape)), "tp", 0, 0, tiled=True
    )
    anywhere = pl.BlockSpec(memory_space=pl.ANY)
    operands = [
        mix_gain[None],
        input_weight,
        branch_weight,
        jnp.swapaxes(conv_state, 0, 1),
        conv_taps,
        conv_bias[None],
        recur_weight,
        recur_bias[None],
        inject_weight,
        inject_bias[None],
        decay_param[None],
        lru_state,
    ]
    half, whole = (quarter // 2, quarter), (quarter // 2 + units, quarter)
    cuts = [whole, whole, half, (units, quarter), half, (units, quarter)]
    cutting = pl.pallas_call(
        functools.partial(cut_weights, members=members),
        out_shape=[jax.ShapeDtypeStruct(shape, BF16) for shape in cuts]
        + [pltpu.VMEM(value.shape, value.dtype) for value in operands],
        in_specs=[SMEM] + [anywhere] * (3 + len(operands)),
        out_specs=[anywhere] * len(cuts) + [VMEM] * len(operands),
        scratch_shapes=[
            pltpu.VMEM((members, *whole), BF16),
            pltpu.SemaphoreType.DMA((members, 5)),
            pltpu.SemaphoreType.DMA((len(cuts),)),
            pltpu.SemaphoreType.DMA((len(operands),)),
        ],
    )
    loaded = cutting(place, expert_gate, expert_up, expert_down, *operands)
    own, across, *sides = loaded[: len(cuts)]
    operands = [near(value) for value in loaded[len(cuts) :]]
    table = pltpu.VMEM((slots, seq_count), BF16)
    ids = route_ids.T
    dispatch, output_near, tokens_near, gain_part = pl.pallas_call(
        dispatch_table,
        out_shape=[
            table,
            pltpu.VMEM(output_weight.shape, BF16),
            pltpu.VMEM(tokens.shape, BF16),
            pltpu.VMEM((1, quarter), F32),
        ],
        in_specs=[SMEM] + [anywhere] * 4,
        out_specs=[VMEM] * 4,
        scratch_shapes=[
            pltpu.VMEM(ids.shape, ids.dtype),
            pltpu.SemaphoreType.DMA((4,)),
        ],
    )(place, ids, output_weight, tokens, moe_gain[None])
    combine_high, combine_low = call(
        combine_tables, [table] * 2, ids, route_logits.T, group_weight[None]
    )
    copies, new_state, window = call(
        mixer,
        [
            pltpu.VMEM((members, seq_count, channels), BF16),
            jax.ShapeDtypeStruct((seq_count, channels), F32),
            jax.ShapeDtypeStruct((conv_state.shape[1], seq_count, channels), BF16),
        ],
        near(token_parts),
        *operands,
    )
    mixer_parts = lax.all_to_all(copies, "tp", 0, 0, tiled=True)

    def onward(value, step):
        ring = [(m, (m + step) % members) for m in range(members)]
        return lax.ppermute(value, "tp", ring)

    across = onward(across, 2)
    cut_next = onward(sides[0], 1)
    cut_last = onward(sides[2], 3)
    down_next = onward(sides[1], 1)
    down_last = onward(sides[3], 3)
    stream, outgoing = call(
        stream_rows,
        [pltpu.VMEM((seq_count, quarter), BF16), pltpu.VMEM((slots, quarter), BF16)],
        near(mixer_parts),
        near(output_near),
        near(tokens_near),
        near(dispatch),
    )

    outgoing = outgoing.reshape(experts, CAPACITY, quarter)
    arrived = lax.all_to_all(outgoing, "ep", 0, 0, tiled=True)
    arrived = arrived.reshape(slots, quarter)
    own, across = near(own), near(across)
    products = call(
        first_products,
        pltpu.VMEM((members, slots + SUM_ROWS, 2 * units), BF16),
        near(arrived),
        near(gain_part),
        own,
        near(cut_next),
        across,
        near(cut_last),
        scalar=place,
    )
    products = lax.all_to_all(products, "tp", 0, 0, tiled=True)
    hidden = call(hidden_units, pltpu.VMEM((members, slots, units), BF16), near(products))
    hidden, down_next, down_last = lax.optimization_barrier((hidden, down_next, down_last))
    hidden = lax.all_to_all(hidden, "tp", 0, 0, tiled=True)
    answer = call(
        last_product,
        pltpu.VMEM((slots, quarter), BF16),
        near(hidden),
        own,
        near(down_next),
        across,
        near(down_last),
        scalar=place,
    )
    returned = lax.all_to_all(answer, "ep", 0, 0, tiled=True)
    routed = dot_on(combine_high, returned, 0, 0) + dot_on(combine_low, returned, 0, 0)
    result = (stream.astype(F32) + routed).astype(BF16)
    return (result, new_state, jnp.swapaxes(window, 0, 1))


def solution(mesh):
    in_specs = (
        P("ep", "tp"),
        P("ep", None, "tp"),
        P("ep", "tp"),
        P(),
        P(None, "tp"),
        P(None, "tp"),
        P(None, "tp"),
        P("tp"),
        P("tp", None, None),
        P("tp"),
        P("tp", None, None),
        P("tp"),
        P("tp"),
        P(None, "tp"),
        P(),
        P("ep", None),
        P("ep", None),
        P("ep"),
        P("ep", None, "tp"),
        P("ep", None, "tp"),
        P("ep", "tp", None),
    )
    out_specs = (P("ep", "tp"), P("ep", "tp"), P("ep", None, "tp"))
    return jax.shard_map(body, mesh=mesh, in_specs=in_specs, out_specs=out_specs, check_vma=False)
```

```python
import functools

import jax
import jax.numpy as jnp
from jax import lax
from jax.experimental import pallas as pl
from jax.experimental.pallas import tpu as pltpu
from jax.sharding import PartitionSpec as P

EPS = 1e-06
RATE = 8.0
CAPACITY = 2
SUM_ROWS = 16
F32 = jnp.float32
BF16 = jnp.bfloat16
VMEM = pl.BlockSpec(memory_space=pltpu.VMEM)
SMEM = pl.BlockSpec(memory_space=pltpu.SMEM)


def near(value):
    return pltpu.with_memory_space_constraint(value, pltpu.VMEM)


def call(kernel, outs, *args, scalar=None):
    scalars = () if scalar is None else (scalar,)
    return pl.pallas_call(
        kernel,
        out_shape=outs,
        in_specs=[SMEM] * len(scalars) + [VMEM] * len(args),
        out_specs=jax.tree.map(lambda _: VMEM, outs),
    )(*scalars, *args)


def dot(a, b):
    return jnp.dot(a, b, preferred_element_type=F32)


def dot_on(a, b, a_dim, b_dim):
    return lax.dot_general(a, b, (((a_dim,), (b_dim,)), ((), ())), preferred_element_type=F32)


def halves(value):
    high = value.astype(BF16)
    return high, (value - high.astype(F32)).astype(BF16)


def places(ids_ref, slots):
    ids = ids_ref[...]
    count = ids.shape[1]
    row = lax.broadcasted_iota(jnp.int32, (slots, count), 0)
    expert = lax.div(row, CAPACITY)
    place = lax.rem(row, CAPACITY)
    first = ids[0:1] == expert
    named = jnp.where(first | (ids[1:2] == expert), 1.0, 0.0)
    before = lax.broadcasted_iota(jnp.int32, (count, count), 0) < lax.broadcasted_iota(
        jnp.int32, (count, count), 1
    )
    earlier = dot(named.astype(BF16), jnp.where(before, 1.0, 0.0).astype(BF16))
    return jnp.where(earlier == place.astype(F32), named, 0.0), first


def dispatch_table(
    member_ref,
    ids_ref,
    weight_ref,
    tokens_ref,
    gain_ref,
    out_ref,
    weight_near_ref,
    tokens_near_ref,
    gain_near_ref,
    ids_near_ref,
    done,
):
    quarter = gain_near_ref.shape[1]
    own = pl.multiple_of(member_ref[0] * quarter, quarter)
    pairs = [
        (ids_ref, ids_near_ref),
        (weight_ref, weight_near_ref),
        (tokens_ref, tokens_near_ref),
        (gain_ref.at[:, pl.ds(own, quarter)], gain_near_ref),
    ]
    copies = [
        pltpu.make_async_copy(source, into, done.at[j]) for j, (source, into) in enumerate(pairs)
    ]
    for copy in copies:
        copy.start()
    copies[0].wait()
    out_ref[...] = places(ids_near_ref, out_ref.shape[0])[0].astype(BF16)
    for copy in copies[1:]:
        copy.wait()


def combine_tables(ids_ref, logits_ref, group_ref, high_ref, low_ref):
    hit, first = places(ids_ref, high_ref.shape[0])
    raised = jnp.exp(logits_ref[...])
    weight = group_ref[...] * raised / (raised[0:1] + raised[1:2])
    high, low = halves(hit * jnp.where(first, weight[0:1], weight[1:2]))
    high_ref[...] = high
    low_ref[...] = low


def cut_weights(member_ref, gate_ref, up_ref, down_ref, *refs, members):
    *rest, piece_ref, reads, writes, loads = refs
    pieces = 2 * members - 2
    count = (len(rest) - pieces) // 2
    far_refs, rest = rest[:count], rest[count:]
    out_refs, near_refs = rest[:pieces], rest[pieces:]
    quarter = gate_ref.shape[1] // members
    half = quarter // 2
    width = gate_ref.shape[2]
    order = (2, 1, 3, 0)
    copies = {}
    for k in order:
        target = lax.rem(member_ref[0] + k, members)
        top = pl.multiple_of(target * quarter, quarter)
        piece = piece_ref.at[k]
        pairs = [(down_ref.at[0, :, pl.ds(top, quarter)], piece.at[pl.ds(half, width), :])]
        for part in range(2):
            rows = pl.ds(pl.multiple_of(top + part * half, half), half)
            at = part * 2 * width
            into = [piece.at[pl.ds(0, half), pl.ds(at + j * width, width)] for j in range(2)]
            pairs += [(gate_ref.at[0, rows, :], into[0]), (up_ref.at[0, rows, :], into[1])]
        copies[k] = [
            pltpu.make_async_copy(source, into, reads.at[k, j])
            for j, (source, into) in enumerate(pairs)
        ]
        for copy in copies[k]:
            copy.start()
    near_copies = [
        pltpu.make_async_copy(source, into, loads.at[j])
        for j, (source, into) in enumerate(zip(far_refs, near_refs))
    ]
    for copy in near_copies:
        copy.start()
    whole = pl.ds(0, half + width)
    parts = [(0, whole), (2, whole)]
    for k in (1, 3):
        parts += [(k, pl.ds(0, half)), (k, pl.ds(half, width))]
    out_copies = []
    for k in order:
        for copy in copies[k]:
            copy.wait()
        for j, (owner, rows) in enumerate(parts):
            if owner == k:
                copy = pltpu.make_async_copy(piece_ref.at[k, rows], out_refs[j], writes.at[j])
                copy.start()
                out_copies.append(copy)
    for copy in near_copies + out_copies:
        copy.wait()


def mixer(
    parts_ref,
    gain_ref,
    input_ref,
    branch_ref,
    conv_ref,
    taps_ref,
    bias_ref,
    recur_ref,
    recur_bias_ref,
    inject_ref,
    inject_bias_ref,
    decay_ref,
    lru_ref,
    copies_ref,
    state_ref,
    window_ref,
):
    members, count, quarter = parts_ref.shape
    taps = taps_ref.shape[0]
    squares = jnp.zeros((count, 1), F32)
    for m in range(members):
        wide = parts_ref[m].astype(F32)
        squares = squares + jnp.sum(wide * wide, axis=1, keepdims=True)
    scale = lax.rsqrt(squares / (members * quarter) + EPS)
    normed = jnp.concatenate(
        [
            (
                parts_ref[m].astype(F32) * scale * gain_ref[:, m * quarter : (m + 1) * quarter]
            ).astype(BF16)
            for m in range(members)
        ],
        axis=1,
    )
    branch_x = dot(normed, input_ref[...]).astype(BF16)
    branch_g = dot(normed, branch_ref[...]).astype(BF16)
    rows = [conv_ref[j] for j in range(taps - 1)] + [branch_x]
    conv_sum = rows[0].astype(F32) * taps_ref[0:1]
    for j in range(1, taps):
        conv_sum = conv_sum + rows[j].astype(F32) * taps_ref[j : j + 1]
        window_ref[j - 1] = rows[j]
    conv_out = (bias_ref[...] + conv_sum).astype(BF16)
    blocks, size, _ = recur_ref.shape

    def gate(weight_ref, gate_bias_ref):
        product = [
            dot(conv_out[:, b * size : (b + 1) * size], weight_ref[b]) for b in range(blocks)
        ]
        return jax.nn.sigmoid(jnp.concatenate(product, axis=1) + gate_bias_ref[...])

    rate = -RATE * jax.nn.softplus(-decay_ref[...])
    log_rate = gate(recur_ref, recur_bias_ref) * rate
    inject = gate(inject_ref, inject_bias_ref)
    kept = jnp.exp(log_rate)
    rest = -jnp.tanh(log_rate) * (1.0 + kept * kept)
    state = kept * lru_ref[...] + jnp.sqrt(rest) * inject * conv_out.astype(F32)
    state_ref[...] = state
    out = (state * jax.nn.gelu(branch_g.astype(F32))).astype(BF16)
    for m in range(members):
        copies_ref[m] = out


def stream_rows(parts_ref, weight_ref, tokens_ref, dispatch_ref, stream_ref, out_ref):
    members, _, width = parts_ref.shape
    mixed = dot(parts_ref[0], weight_ref[:width, :])
    for m in range(1, members):
        mixed = mixed + dot(parts_ref[m], weight_ref[m * width : (m + 1) * width, :])
    stream = (tokens_ref[...].astype(F32) + mixed).astype(BF16)
    stream_ref[...] = stream
    out_ref[...] = dot(dispatch_ref[...], stream).astype(BF16).reshape(out_ref.shape)


def first_products(member_ref, rows_ref, gain_ref, *refs):
    *weight_refs, out_ref = refs
    members = len(weight_refs)
    count, width = rows_ref.shape
    half = width // 2
    owners = [lax.rem(member_ref[0] + (members - k), members) for k in range(members)]
    rows = rows_ref[...].astype(F32)
    scaled = (rows * gain_ref[...]).astype(BF16)
    squares = rows * rows
    high, low = halves(squares)
    ones = jnp.ones((SUM_ROWS, width), BF16)
    sums_high, sums_low = halves(dot_on(ones, high, 1, 1) + dot_on(ones, low, 1, 1))
    place = lax.broadcasted_iota(jnp.int32, (SUM_ROWS, count), 0)
    sums = jnp.where(
        place == 0, sums_high.astype(F32), jnp.where(place == 1, sums_low.astype(F32), 0.0)
    ).astype(BF16)
    for k in range(members):
        out_ref[k, count:, :] = sums
    for k, cut in enumerate(weight_refs):
        product = dot(scaled[:, :half], cut[:half, :half]) + dot(
            scaled[:, half:], cut[:half, half:]
        )
        out_ref[owners[k], :count, :] = product.astype(BF16)


def hidden_units(parts_ref, out_ref):
    members, total, width = parts_ref.shape
    count = total - SUM_ROWS
    half = width // 2
    product = parts_ref[0, :count, :].astype(F32)
    sums = parts_ref[0, count:, :].astype(F32)
    for k in range(1, members):
        product = product + parts_ref[k, :count, :].astype(F32)
        sums = sums + parts_ref[k, count:, :].astype(F32)
    row_sum = jnp.sum(jnp.transpose(sums), axis=1, keepdims=True)
    product = product * lax.rsqrt(row_sum / (members * 2 * width) + EPS)
    gate = product[:, :half]
    hidden = (gate * jax.nn.sigmoid(gate) * product[:, half:]).astype(BF16)
    for k in range(members):
        out_ref[k] = hidden


def last_product(member_ref, hidden_ref, *refs):
    *weight_refs, out_ref = refs
    members, _, width = hidden_ref.shape
    total = jnp.zeros((hidden_ref.shape[1], out_ref.shape[-1]), F32)
    for k, weight_ref in enumerate(weight_refs):
        owner = lax.rem(member_ref[0] + (members - k), members)
        total = total + dot(hidden_ref[owner], weight_ref[weight_ref.shape[0] - width :, :])
    out_ref[...] = total.astype(BF16).reshape(out_ref.shape)


def add_routed(back_ref, high_ref, low_ref, stream_ref, out_ref):
    back = back_ref[...].reshape(high_ref.shape[0], -1)
    routed = dot_on(high_ref[...], back, 0, 0) + dot_on(low_ref[...], back, 0, 0)
    out_ref[...] = (stream_ref[...].astype(F32) + routed).astype(BF16)


def body(
    tokens,
    conv_state,
    lru_state,
    mix_gain,
    input_weight,
    branch_weight,
    conv_taps,
    conv_bias,
    recur_weight,
    recur_bias,
    inject_weight,
    inject_bias,
    decay_param,
    output_weight,
    moe_gain,
    route_ids,
    route_logits,
    group_weight,
    expert_gate,
    expert_up,
    expert_down,
):
    seq_count, quarter = tokens.shape
    channels = lru_state.shape[1]
    members = lax.axis_size("tp")
    experts = lax.axis_size("ep")
    member = lax.axis_index("tp")
    place = member.astype(jnp.int32)[None]
    slots = experts * CAPACITY
    units = expert_gate.shape[2]

    token_parts = lax.all_to_all(
        jnp.broadcast_to(tokens[None], (members, *tokens.shape)), "tp", 0, 0, tiled=True
    )
    anywhere = pl.BlockSpec(memory_space=pl.ANY)
    operands = [
        mix_gain[None],
        input_weight,
        branch_weight,
        jnp.swapaxes(conv_state, 0, 1),
        conv_taps,
        conv_bias[None],
        recur_weight,
        recur_bias[None],
        inject_weight,
        inject_bias[None],
        decay_param[None],
        lru_state,
    ]
    half, whole = (quarter // 2, quarter), (quarter // 2 + units, quarter)
    cuts = [whole, whole, half, (units, quarter), half, (units, quarter)]
    cutting = pl.pallas_call(
        functools.partial(cut_weights, members=members),
        out_shape=[jax.ShapeDtypeStruct(shape, BF16) for shape in cuts]
        + [pltpu.VMEM(value.shape, value.dtype) for value in operands],
        in_specs=[SMEM] + [anywhere] * (3 + len(operands)),
        out_specs=[anywhere] * len(cuts) + [VMEM] * len(operands),
        scratch_shapes=[
            pltpu.VMEM((members, *whole), BF16),
            pltpu.SemaphoreType.DMA((members, 5)),
            pltpu.SemaphoreType.DMA((len(cuts),)),
            pltpu.SemaphoreType.DMA((len(operands),)),
        ],
    )
    loaded = cutting(place, expert_gate, expert_up, expert_down, *operands)
    own, across, *sides = loaded[: len(cuts)]
    operands = [near(value) for value in loaded[len(cuts) :]]
    table = pltpu.VMEM((slots, seq_count), BF16)
    ids = route_ids.T
    dispatch, output_near, tokens_near, gain_part = pl.pallas_call(
        dispatch_table,
        out_shape=[
            table,
            pltpu.VMEM(output_weight.shape, BF16),
            pltpu.VMEM(tokens.shape, BF16),
            pltpu.VMEM((1, quarter), F32),
        ],
        in_specs=[SMEM] + [anywhere] * 4,
        out_specs=[VMEM] * 4,
        scratch_shapes=[
            pltpu.VMEM(ids.shape, ids.dtype),
            pltpu.SemaphoreType.DMA((4,)),
        ],
    )(place, ids, output_weight, tokens, moe_gain[None])
    combine_high, combine_low = call(
        combine_tables, [table] * 2, ids, route_logits.T, group_weight[None]
    )
    copies, new_state, window = call(
        mixer,
        [
            pltpu.VMEM((members, seq_count, channels), BF16),
            jax.ShapeDtypeStruct((seq_count, channels), F32),
            jax.ShapeDtypeStruct((conv_state.shape[1], seq_count, channels), BF16),
        ],
        near(token_parts),
        *operands,
    )
    mixer_parts = lax.all_to_all(copies, "tp", 0, 0, tiled=True)

    def onward(value, step):
        ring = [(m, (m + step) % members) for m in range(members)]
        return lax.ppermute(value, "tp", ring)

    across = onward(across, 2)
    cut_next = onward(sides[0], 1)
    cut_last = onward(sides[2], 3)
    down_next = onward(sides[1], 1)
    down_last = onward(sides[3], 3)
    stream, outgoing = call(
        stream_rows,
        [
            pltpu.VMEM((seq_count, quarter), BF16),
            jax.ShapeDtypeStruct((experts, CAPACITY, quarter), BF16),
        ],
        near(mixer_parts),
        near(output_near),
        near(tokens_near),
        near(dispatch),
    )

    arrived = lax.all_to_all(outgoing, "ep", 0, 0, tiled=True)
    arrived = arrived.reshape(slots, quarter)
    own, across = near(own), near(across)
    products = call(
        first_products,
        pltpu.VMEM((members, slots + SUM_ROWS, 2 * units), BF16),
        near(arrived),
        near(gain_part),
        own,
        near(cut_next),
        across,
        near(cut_last),
        scalar=place,
    )
    products = lax.all_to_all(products, "tp", 0, 0, tiled=True)
    hidden = call(hidden_units, pltpu.VMEM((members, slots, units), BF16), near(products))
    hidden, down_next, down_last = lax.optimization_barrier((hidden, down_next, down_last))
    hidden = lax.all_to_all(hidden, "tp", 0, 0, tiled=True)
    answer = call(
        last_product,
        pltpu.VMEM((experts, CAPACITY, quarter), BF16),
        near(hidden),
        own,
        near(down_next),
        across,
        near(down_last),
        scalar=place,
    )
    returned = lax.all_to_all(answer, "ep", 0, 0, tiled=True)
    result = call(
        add_routed,
        jax.ShapeDtypeStruct((seq_count, quarter), BF16),
        near(returned),
        near(combine_high),
        near(combine_low),
        near(stream),
    )
    return (result, new_state, jnp.swapaxes(window, 0, 1))


def solution(mesh):
    in_specs = (
        P("ep", "tp"),
        P("ep", None, "tp"),
        P("ep", "tp"),
        P(),
        P(None, "tp"),
        P(None, "tp"),
        P(None, "tp"),
        P("tp"),
        P("tp", None, None),
        P("tp"),
        P("tp", None, None),
        P("tp"),
        P("tp"),
        P(None, "tp"),
        P(),
        P("ep", None),
        P("ep", None),
        P("ep"),
        P("ep", None, "tp"),
        P("ep", None, "tp"),
        P("ep", "tp", None),
    )
    out_specs = (P("ep", "tp"), P("ep", "tp"), P("ep", None, "tp"))
    return jax.shard_map(body, mesh=mesh, in_specs=in_specs, out_specs=out_specs, check_vma=False)
```

```python
import functools

import jax
import jax.numpy as jnp
from jax import lax
from jax.experimental import pallas as pl
from jax.experimental.pallas import tpu as pltpu
from jax.sharding import Mesh
from jax.sharding import PartitionSpec as P

EPS = 1e-06
RATE = 8.0
CAPACITY = 2
SUM_ROWS = 16
CORES = 2
EP = ("z", "x", "core")
F32 = jnp.float32
BF16 = jnp.bfloat16
VMEM = pl.BlockSpec(memory_space=pltpu.VMEM)
SMEM = pl.BlockSpec(memory_space=pltpu.SMEM)


def near(value):
    return pltpu.with_memory_space_constraint(value, pltpu.VMEM)


def call(kernel, outs, *args, scalar=None):
    scalars = () if scalar is None else (scalar,)
    return pl.pallas_call(
        kernel,
        out_shape=outs,
        in_specs=[SMEM] * len(scalars) + [VMEM] * len(args),
        out_specs=jax.tree.map(lambda _: VMEM, outs),
    )(*scalars, *args)


def dot(a, b):
    return jnp.dot(a, b, preferred_element_type=F32)


def dot_on(a, b, a_dim, b_dim):
    return lax.dot_general(a, b, (((a_dim,), (b_dim,)), ((), ())), preferred_element_type=F32)


def halves(value):
    high = value.astype(BF16)
    return high, (value - high.astype(F32)).astype(BF16)


def places(ids_ref, slots):
    ids = ids_ref[...]
    count = ids.shape[1]
    row = lax.broadcasted_iota(jnp.int32, (slots, count), 0)
    expert = lax.div(row, CAPACITY)
    place = lax.rem(row, CAPACITY)
    first = ids[0:1] == expert
    named = jnp.where(first | (ids[1:2] == expert), 1.0, 0.0)
    before = lax.broadcasted_iota(jnp.int32, (count, count), 0) < lax.broadcasted_iota(
        jnp.int32, (count, count), 1
    )
    earlier = dot(named.astype(BF16), jnp.where(before, 1.0, 0.0).astype(BF16))
    return jnp.where(earlier == place.astype(F32), named, 0.0), first


def dispatch_table(
    member_ref,
    ids_ref,
    weight_ref,
    tokens_ref,
    gain_ref,
    out_ref,
    weight_near_ref,
    tokens_near_ref,
    gain_near_ref,
    ids_near_ref,
    done,
):
    quarter = gain_near_ref.shape[1]
    own = pl.multiple_of(member_ref[0] * quarter, quarter)
    pairs = [
        (ids_ref, ids_near_ref),
        (weight_ref, weight_near_ref),
        (tokens_ref, tokens_near_ref),
        (gain_ref.at[:, pl.ds(own, quarter)], gain_near_ref),
    ]
    copies = [
        pltpu.make_async_copy(source, into, done.at[j]) for j, (source, into) in enumerate(pairs)
    ]
    for copy in copies:
        copy.start()
    copies[0].wait()
    out_ref[...] = places(ids_near_ref, out_ref.shape[0])[0].astype(BF16)
    for copy in copies[1:]:
        copy.wait()


def combine_tables(ids_ref, logits_ref, group_ref, high_ref, low_ref):
    hit, first = places(ids_ref, high_ref.shape[0])
    raised = jnp.exp(logits_ref[...])
    weight = group_ref[...] * raised / (raised[0:1] + raised[1:2])
    high, low = halves(hit * jnp.where(first, weight[0:1], weight[1:2]))
    high_ref[...] = high
    low_ref[...] = low


def cut_weights(member_ref, gate_ref, up_ref, down_ref, *refs, members):
    *rest, piece_ref, reads, writes, loads = refs
    pieces = 2 * members - 2
    count = (len(rest) - pieces) // 2
    far_refs, rest = rest[:count], rest[count:]
    out_refs, near_refs = rest[:pieces], rest[pieces:]
    quarter = gate_ref.shape[1] // members
    half = quarter // 2
    width = gate_ref.shape[2]
    order = (2, 1, 3, 0)
    copies = {}
    for k in order:
        target = lax.rem(member_ref[0] + k, members)
        top = pl.multiple_of(target * quarter, quarter)
        piece = piece_ref.at[k]
        pairs = [(down_ref.at[0, :, pl.ds(top, quarter)], piece.at[pl.ds(half, width), :])]
        for part in range(2):
            rows = pl.ds(pl.multiple_of(top + part * half, half), half)
            at = part * 2 * width
            into = [piece.at[pl.ds(0, half), pl.ds(at + j * width, width)] for j in range(2)]
            pairs += [(gate_ref.at[0, rows, :], into[0]), (up_ref.at[0, rows, :], into[1])]
        copies[k] = [
            pltpu.make_async_copy(source, into, reads.at[k, j])
            for j, (source, into) in enumerate(pairs)
        ]
        for copy in copies[k]:
            copy.start()
    near_copies = [
        pltpu.make_async_copy(source, into, loads.at[j])
        for j, (source, into) in enumerate(zip(far_refs, near_refs))
    ]
    for copy in near_copies:
        copy.start()
    whole = pl.ds(0, half + width)
    parts = [(0, whole), (2, whole)]
    for k in (1, 3):
        parts += [(k, pl.ds(0, half)), (k, pl.ds(half, width))]
    out_copies = []
    for k in order:
        for copy in copies[k]:
            copy.wait()
        for j, (owner, rows) in enumerate(parts):
            if owner == k:
                copy = pltpu.make_async_copy(piece_ref.at[k, rows], out_refs[j], writes.at[j])
                copy.start()
                out_copies.append(copy)
    for copy in near_copies + out_copies:
        copy.wait()


def mixer(
    parts_ref,
    gain_ref,
    input_ref,
    branch_ref,
    conv_ref,
    taps_ref,
    bias_ref,
    recur_ref,
    recur_bias_ref,
    inject_ref,
    inject_bias_ref,
    decay_ref,
    lru_ref,
    copies_ref,
    state_ref,
    window_ref,
):
    members, count, quarter = parts_ref.shape
    taps = taps_ref.shape[0]
    squares = jnp.zeros((count, 1), F32)
    for m in range(members):
        wide = parts_ref[m].astype(F32)
        squares = squares + jnp.sum(wide * wide, axis=1, keepdims=True)
    scale = lax.rsqrt(squares / (members * quarter) + EPS)
    normed = jnp.concatenate(
        [
            (
                parts_ref[m].astype(F32) * scale * gain_ref[:, m * quarter : (m + 1) * quarter]
            ).astype(BF16)
            for m in range(members)
        ],
        axis=1,
    )
    branch_x = dot(normed, input_ref[...]).astype(BF16)
    branch_g = dot(normed, branch_ref[...]).astype(BF16)
    rows = [conv_ref[j] for j in range(taps - 1)] + [branch_x]
    conv_sum = rows[0].astype(F32) * taps_ref[0:1]
    for j in range(1, taps):
        conv_sum = conv_sum + rows[j].astype(F32) * taps_ref[j : j + 1]
        window_ref[j - 1] = rows[j]
    conv_out = (bias_ref[...] + conv_sum).astype(BF16)
    blocks, size, _ = recur_ref.shape

    def gate(weight_ref, gate_bias_ref):
        product = [
            dot(conv_out[:, b * size : (b + 1) * size], weight_ref[b]) for b in range(blocks)
        ]
        return jax.nn.sigmoid(jnp.concatenate(product, axis=1) + gate_bias_ref[...])

    rate = -RATE * jax.nn.softplus(-decay_ref[...])
    log_rate = gate(recur_ref, recur_bias_ref) * rate
    inject = gate(inject_ref, inject_bias_ref)
    kept = jnp.exp(log_rate)
    rest = -jnp.tanh(log_rate) * (1.0 + kept * kept)
    state = kept * lru_ref[...] + jnp.sqrt(rest) * inject * conv_out.astype(F32)
    state_ref[...] = state
    out = (state * jax.nn.gelu(branch_g.astype(F32))).astype(BF16)
    for m in range(members):
        copies_ref[m] = out


def stream_rows(parts_ref, weight_ref, tokens_ref, dispatch_ref, stream_ref, out_ref):
    members, _, width = parts_ref.shape
    mixed = dot(parts_ref[0], weight_ref[:width, :])
    for m in range(1, members):
        mixed = mixed + dot(parts_ref[m], weight_ref[m * width : (m + 1) * width, :])
    stream = (tokens_ref[...].astype(F32) + mixed).astype(BF16)
    stream_ref[...] = stream
    out_ref[...] = dot(dispatch_ref[...], stream).astype(BF16).reshape(out_ref.shape)


def first_products(member_ref, rows_ref, gain_ref, *refs):
    *weight_refs, out_ref = refs
    members = len(weight_refs)
    width = rows_ref.shape[-1]
    count = out_ref.shape[1] - SUM_ROWS
    half = width // 2
    shape = (count, count * CORES)
    row = lax.broadcasted_iota(jnp.int32, shape, 0)
    column = lax.broadcasted_iota(jnp.int32, shape, 1)
    chip = lax.div(row, CORES * CAPACITY)
    sender = lax.rem(lax.div(row, CAPACITY), CORES)
    source = sender * count + (chip * CORES + member_ref[1]) * CAPACITY + lax.rem(row, CAPACITY)
    choice = jnp.where(column == source, 1.0, 0.0).astype(BF16)
    owners = [lax.rem(member_ref[0] + (members - k), members) for k in range(members)]
    rows = dot(choice, rows_ref[...].reshape(count * CORES, width))
    scaled = (rows * gain_ref[...]).astype(BF16)
    squares = rows * rows
    high, low = halves(squares)
    ones = jnp.ones((SUM_ROWS, width), BF16)
    sums_high, sums_low = halves(dot_on(ones, high, 1, 1) + dot_on(ones, low, 1, 1))
    place = lax.broadcasted_iota(jnp.int32, (SUM_ROWS, count), 0)
    sums = jnp.where(
        place == 0, sums_high.astype(F32), jnp.where(place == 1, sums_low.astype(F32), 0.0)
    ).astype(BF16)
    for k in range(members):
        out_ref[k, count:, :] = sums
    for k, cut in enumerate(weight_refs):
        product = dot(scaled[:, :half], cut[:half, :half]) + dot(
            scaled[:, half:], cut[:half, half:]
        )
        out_ref[owners[k], :count, :] = product.astype(BF16)


def hidden_units(parts_ref, out_ref):
    members, total, width = parts_ref.shape
    count = total - SUM_ROWS
    half = width // 2
    product = parts_ref[0, :count, :].astype(F32)
    sums = parts_ref[0, count:, :].astype(F32)
    for k in range(1, members):
        product = product + parts_ref[k, :count, :].astype(F32)
        sums = sums + parts_ref[k, count:, :].astype(F32)
    row_sum = jnp.sum(jnp.transpose(sums), axis=1, keepdims=True)
    product = product * lax.rsqrt(row_sum / (members * 2 * width) + EPS)
    gate = product[:, :half]
    hidden = (gate * jax.nn.sigmoid(gate) * product[:, half:]).astype(BF16)
    for k in range(members):
        out_ref[k] = hidden


def last_product(member_ref, hidden_ref, *refs):
    *weight_refs, out_ref = refs
    members, _, width = hidden_ref.shape
    total = jnp.zeros((hidden_ref.shape[1], out_ref.shape[-1]), F32)
    for k, weight_ref in enumerate(weight_refs):
        owner = lax.rem(member_ref[0] + (members - k), members)
        total = total + dot(hidden_ref[owner], weight_ref[weight_ref.shape[0] - width :, :])
    out_ref[...] = total.astype(BF16).reshape(out_ref.shape)


def add_routed(back_ref, high_ref, low_ref, stream_ref, out_ref):
    back = back_ref[...].reshape(high_ref.shape[0], -1)
    routed = dot_on(high_ref[...], back, 0, 0) + dot_on(low_ref[...], back, 0, 0)
    out_ref[...] = (stream_ref[...].astype(F32) + routed).astype(BF16)


def body(
    tokens,
    conv_state,
    lru_state,
    mix_gain,
    input_weight,
    branch_weight,
    conv_taps,
    conv_bias,
    recur_weight,
    recur_bias,
    inject_weight,
    inject_bias,
    decay_param,
    output_weight,
    moe_gain,
    route_ids,
    route_logits,
    group_weight,
    expert_gate,
    expert_up,
    expert_down,
):
    seq_count, quarter = tokens.shape
    channels = lru_state.shape[1]
    members = lax.axis_size("tp")
    experts = lax.axis_size("z") * lax.axis_size("x") * CORES
    core = lax.axis_index("core").astype(jnp.int32)
    member = lax.axis_index("tp")
    place = member.astype(jnp.int32)[None]
    slots = experts * CAPACITY
    units = expert_gate.shape[2]

    token_parts = lax.all_to_all(
        jnp.broadcast_to(tokens[None], (members, *tokens.shape)), "tp", 0, 0, tiled=True
    )
    anywhere = pl.BlockSpec(memory_space=pl.ANY)
    operands = [
        mix_gain[None],
        input_weight,
        branch_weight,
        jnp.swapaxes(conv_state, 0, 1),
        conv_taps,
        conv_bias[None],
        recur_weight,
        recur_bias[None],
        inject_weight,
        inject_bias[None],
        decay_param[None],
        lru_state,
    ]
    half, whole = (quarter // 2, quarter), (quarter // 2 + units, quarter)
    cuts = [whole, whole, half, (units, quarter), half, (units, quarter)]
    cutting = pl.pallas_call(
        functools.partial(cut_weights, members=members),
        out_shape=[jax.ShapeDtypeStruct(shape, BF16) for shape in cuts]
        + [pltpu.VMEM(value.shape, value.dtype) for value in operands],
        in_specs=[SMEM] + [anywhere] * (3 + len(operands)),
        out_specs=[anywhere] * len(cuts) + [VMEM] * len(operands),
        scratch_shapes=[
            pltpu.VMEM((members, *whole), BF16),
            pltpu.SemaphoreType.DMA((members, 5)),
            pltpu.SemaphoreType.DMA((len(cuts),)),
            pltpu.SemaphoreType.DMA((len(operands),)),
        ],
    )
    loaded = cutting(place, expert_gate, expert_up, expert_down, *operands)
    own, across, *sides = loaded[: len(cuts)]
    operands = [near(value) for value in loaded[len(cuts) :]]
    table = pltpu.VMEM((slots, seq_count), BF16)
    ids = route_ids.T
    dispatch, output_near, tokens_near, gain_part = pl.pallas_call(
        dispatch_table,
        out_shape=[
            table,
            pltpu.VMEM(output_weight.shape, BF16),
            pltpu.VMEM(tokens.shape, BF16),
            pltpu.VMEM((1, quarter), F32),
        ],
        in_specs=[SMEM] + [anywhere] * 4,
        out_specs=[VMEM] * 4,
        scratch_shapes=[
            pltpu.VMEM(ids.shape, ids.dtype),
            pltpu.SemaphoreType.DMA((4,)),
        ],
    )(place, ids, output_weight, tokens, moe_gain[None])
    combine_high, combine_low = call(
        combine_tables, [table] * 2, ids, route_logits.T, group_weight[None]
    )
    copies, new_state, window = call(
        mixer,
        [
            pltpu.VMEM((members, seq_count, channels), BF16),
            jax.ShapeDtypeStruct((seq_count, channels), F32),
            jax.ShapeDtypeStruct((conv_state.shape[1], seq_count, channels), BF16),
        ],
        near(token_parts),
        *operands,
    )
    mixer_parts = lax.all_to_all(copies, "tp", 0, 0, tiled=True)

    def onward(value, step):
        ring = [(m, (m + step) % members) for m in range(members)]
        return lax.ppermute(value, "tp", ring)

    across = onward(across, 2)
    cut_next = onward(sides[0], 1)
    cut_last = onward(sides[2], 3)
    down_next = onward(sides[1], 1)
    down_last = onward(sides[3], 3)
    stream, outgoing = call(
        stream_rows,
        [
            pltpu.VMEM((seq_count, quarter), BF16),
            jax.ShapeDtypeStruct((experts // CORES, CORES * CAPACITY, quarter), BF16),
        ],
        near(mixer_parts),
        near(output_near),
        near(tokens_near),
        near(dispatch),
    )

    arrived = lax.all_to_all(outgoing, ("z", "x"), 0, 0, tiled=True)
    arrived = lax.all_gather(arrived, "core", axis=0, tiled=True)
    own, across = near(own), near(across)
    products = call(
        first_products,
        pltpu.VMEM((members, slots + SUM_ROWS, 2 * units), BF16),
        near(arrived),
        near(gain_part),
        own,
        near(cut_next),
        across,
        near(cut_last),
        scalar=jnp.stack([place[0], core]),
    )
    products = lax.all_to_all(products, "tp", 0, 0, tiled=True)
    hidden = call(hidden_units, pltpu.VMEM((members, slots, units), BF16), near(products))
    hidden, down_next, down_last = lax.optimization_barrier((hidden, down_next, down_last))
    hidden = lax.all_to_all(hidden, "tp", 0, 0, tiled=True)
    answer = call(
        last_product,
        pltpu.VMEM((experts, CAPACITY, quarter), BF16),
        near(hidden),
        own,
        near(down_next),
        across,
        near(down_last),
        scalar=place,
    )
    returned = lax.all_to_all(answer, EP, 0, 0, tiled=True)
    result = call(
        add_routed,
        jax.ShapeDtypeStruct((seq_count, quarter), BF16),
        near(returned),
        near(combine_high),
        near(combine_low),
        near(stream),
    )
    return (result, new_state, jnp.swapaxes(window, 0, 1))


def solution(mesh):
    in_specs = (
        P(EP, "tp"),
        P(EP, None, "tp"),
        P(EP, "tp"),
        P(),
        P(None, "tp"),
        P(None, "tp"),
        P(None, "tp"),
        P("tp"),
        P("tp", None, None),
        P("tp"),
        P("tp", None, None),
        P("tp"),
        P("tp"),
        P(None, "tp"),
        P(),
        P(EP, None),
        P(EP, None),
        P(EP),
        P(EP, None, "tp"),
        P(EP, None, "tp"),
        P(EP, "tp", None),
    )
    out_specs = (P(EP, "tp"), P(EP, "tp"), P(EP, None, "tp"))
    members = mesh.shape["tp"]
    _, members = mesh.devices.shape
    chips = mesh.devices.reshape(-1, 4, CORES, members)
    return jax.shard_map(
        body,
        mesh=Mesh(chips, (*EP, "tp")),
        in_specs=in_specs,
        out_specs=out_specs,
        check_vma=False,
    )
```

```python
import functools

import jax
import jax.numpy as jnp
from jax import lax
from jax.experimental import pallas as pl
from jax.experimental.pallas import tpu as pltpu
from jax.sharding import PartitionSpec as P

EPS = 1e-06
RATE = 8.0
CAPACITY = 2
SUM_ROWS = 16
F32 = jnp.float32
BF16 = jnp.bfloat16
VMEM = pl.BlockSpec(memory_space=pltpu.VMEM)
SMEM = pl.BlockSpec(memory_space=pltpu.SMEM)


def near(value):
    return pltpu.with_memory_space_constraint(value, pltpu.VMEM)


def call(kernel, outs, *args, scalar=None):
    scalars = () if scalar is None else (scalar,)
    return pl.pallas_call(
        kernel,
        out_shape=outs,
        in_specs=[SMEM] * len(scalars) + [VMEM] * len(args),
        out_specs=jax.tree.map(lambda _: VMEM, outs),
    )(*scalars, *args)


def dot(a, b):
    return jnp.dot(a, b, preferred_element_type=F32)


def dot_on(a, b, a_dim, b_dim):
    return lax.dot_general(a, b, (((a_dim,), (b_dim,)), ((), ())), preferred_element_type=F32)


def halves(value):
    high = value.astype(BF16)
    return high, (value - high.astype(F32)).astype(BF16)


def places(ids_ref, slots):
    ids = ids_ref[...]
    count = ids.shape[1]
    row = lax.broadcasted_iota(jnp.int32, (slots, count), 0)
    expert = lax.div(row, CAPACITY)
    place = lax.rem(row, CAPACITY)
    first = ids[0:1] == expert
    named = jnp.where(first | (ids[1:2] == expert), 1.0, 0.0)
    before = lax.broadcasted_iota(jnp.int32, (count, count), 0) < lax.broadcasted_iota(
        jnp.int32, (count, count), 1
    )
    earlier = dot(named.astype(BF16), jnp.where(before, 1.0, 0.0).astype(BF16))
    return jnp.where(earlier == place.astype(F32), named, 0.0), first


def combine_tables(
    feature_ref, ids_ref, logits_ref, group_ref, gain_ref, high_ref, low_ref, gain_near_ref, done
):
    width = gain_near_ref.shape[1]
    own = pl.multiple_of(feature_ref[0], width)
    copy = pltpu.make_async_copy(gain_ref.at[:, pl.ds(own, width)], gain_near_ref, done)
    copy.start()
    hit, first = places(ids_ref, high_ref.shape[0])
    raised = jnp.exp(logits_ref[...])
    weight = group_ref[...] * raised / (raised[0:1] + raised[1:2])
    high, low = halves(hit * jnp.where(first, weight[0:1], weight[1:2]))
    high_ref[...] = high
    low_ref[...] = low
    copy.wait()


def cut_weights(member_ref, ids_ref, gate_ref, up_ref, down_ref, *refs, members):
    *rest, table_ref, piece_ref, ids_near_ref, reads, writes, loads = refs
    pieces = 2 * members - 2
    count = (len(rest) - pieces) // 2
    far_refs, rest = rest[:count], rest[count:]
    out_refs, near_refs = rest[:pieces], rest[pieces:]
    quarter = gate_ref.shape[1] // members
    half = quarter // 2
    width = gate_ref.shape[2]
    order = (2, 1, 3, 0)
    ids_copy = pltpu.make_async_copy(ids_ref, ids_near_ref, loads.at[count])
    ids_copy.start()
    copies = {}
    for k in order:
        target = lax.rem(member_ref[0] + k, members)
        top = pl.multiple_of(target * quarter, quarter)
        piece = piece_ref.at[k]
        pairs = [(down_ref.at[0, :, pl.ds(top, quarter)], piece.at[pl.ds(half, width), :])]
        for part in range(2):
            rows = pl.ds(pl.multiple_of(top + part * half, half), half)
            at = part * 2 * width
            into = [piece.at[pl.ds(0, half), pl.ds(at + j * width, width)] for j in range(2)]
            pairs += [(gate_ref.at[0, rows, :], into[0]), (up_ref.at[0, rows, :], into[1])]
        copies[k] = [
            pltpu.make_async_copy(source, into, reads.at[k, j])
            for j, (source, into) in enumerate(pairs)
        ]
        for copy in copies[k]:
            copy.start()
    near_copies = [
        pltpu.make_async_copy(source, into, loads.at[j])
        for j, (source, into) in enumerate(zip(far_refs, near_refs))
    ]
    for copy in near_copies:
        copy.start()
    whole = pl.ds(0, half + width)
    parts = [(0, whole), (2, whole)]
    for k in (1, 3):
        parts += [(k, pl.ds(0, half)), (k, pl.ds(half, width))]
    ids_copy.wait()
    table_ref[...] = places(ids_near_ref, table_ref.shape[0])[0].astype(BF16)
    out_copies = []
    for k in order:
        for copy in copies[k]:
            copy.wait()
        for j, (owner, rows) in enumerate(parts):
            if owner == k:
                copy = pltpu.make_async_copy(piece_ref.at[k, rows], out_refs[j], writes.at[j])
                copy.start()
                out_copies.append(copy)
    for copy in near_copies + out_copies:
        copy.wait()


def mixer(
    parts_ref,
    gain_ref,
    input_ref,
    branch_ref,
    conv_ref,
    taps_ref,
    bias_ref,
    recur_ref,
    recur_bias_ref,
    inject_ref,
    inject_bias_ref,
    decay_ref,
    lru_ref,
    copies_ref,
    state_ref,
    window_ref,
):
    members, count, quarter = parts_ref.shape
    taps = taps_ref.shape[0]
    squares = jnp.zeros((count, 1), F32)
    for m in range(members):
        wide = parts_ref[m].astype(F32)
        squares = squares + jnp.sum(wide * wide, axis=1, keepdims=True)
    scale = lax.rsqrt(squares / (members * quarter) + EPS)
    normed = jnp.concatenate(
        [
            (
                parts_ref[m].astype(F32) * scale * gain_ref[:, m * quarter : (m + 1) * quarter]
            ).astype(BF16)
            for m in range(members)
        ],
        axis=1,
    )
    branch_x = dot(normed, input_ref[...]).astype(BF16)
    branch_g = dot(normed, branch_ref[...]).astype(BF16)
    rows = [conv_ref[j] for j in range(taps - 1)] + [branch_x]
    conv_sum = rows[0].astype(F32) * taps_ref[0:1]
    for j in range(1, taps):
        conv_sum = conv_sum + rows[j].astype(F32) * taps_ref[j : j + 1]
        window_ref[j - 1] = rows[j]
    conv_out = (bias_ref[...] + conv_sum).astype(BF16)
    blocks, size, _ = recur_ref.shape

    def gate(weight_ref, gate_bias_ref):
        product = [
            dot(conv_out[:, b * size : (b + 1) * size], weight_ref[b]) for b in range(blocks)
        ]
        return jax.nn.sigmoid(jnp.concatenate(product, axis=1) + gate_bias_ref[...])

    rate = -RATE * jax.nn.softplus(-decay_ref[...])
    log_rate = gate(recur_ref, recur_bias_ref) * rate
    inject = gate(inject_ref, inject_bias_ref)
    kept = jnp.exp(log_rate)
    rest = -jnp.tanh(log_rate) * (1.0 + kept * kept)
    state = kept * lru_ref[...] + jnp.sqrt(rest) * inject * conv_out.astype(F32)
    state_ref[...] = state
    out = (state * jax.nn.gelu(branch_g.astype(F32))).astype(BF16)
    for m in range(members):
        copies_ref[m] = out


def stream_rows(
    parts_ref, dispatch_ref, weight_ref, tokens_ref, stream_ref, out_ref, near_ref, tokens_near_ref, done
):
    members, _, width = parts_ref.shape
    copies = [
        pltpu.make_async_copy(
            weight_ref.at[pl.ds(m * width, width), :],
            near_ref.at[pl.ds(m * width, width), :],
            done.at[m],
        )
        for m in range(members)
    ]
    copies.append(pltpu.make_async_copy(tokens_ref, tokens_near_ref, done.at[members]))
    for copy in copies:
        copy.start()
    mixed = jnp.zeros(stream_ref.shape, F32)
    for m in range(members):
        copies[m].wait()
        mixed = mixed + dot(parts_ref[m], near_ref[m * width : (m + 1) * width, :])
    copies[members].wait()
    stream = (tokens_near_ref[...].astype(F32) + mixed).astype(BF16)
    stream_ref[...] = stream
    out_ref[...] = dot(dispatch_ref[...], stream).astype(BF16).reshape(out_ref.shape)


def first_products(member_ref, rows_ref, gain_ref, *refs):
    *weight_refs, out_ref = refs
    members = len(weight_refs)
    count, width = rows_ref.shape
    half = width // 2
    owners = [lax.rem(member_ref[0] + (members - k), members) for k in range(members)]
    rows = rows_ref[...].astype(F32)
    scaled = (rows * gain_ref[...]).astype(BF16)
    squares = rows * rows
    high, low = halves(squares)
    ones = jnp.ones((SUM_ROWS, width), BF16)
    sums_high, sums_low = halves(dot_on(ones, high, 1, 1) + dot_on(ones, low, 1, 1))
    place = lax.broadcasted_iota(jnp.int32, (SUM_ROWS, count), 0)
    sums = jnp.where(
        place == 0, sums_high.astype(F32), jnp.where(place == 1, sums_low.astype(F32), 0.0)
    ).astype(BF16)
    for k in range(members):
        out_ref[k, count:, :] = sums
    for k, cut in enumerate(weight_refs):
        product = dot(scaled[:, :half], cut[:half, :half]) + dot(
            scaled[:, half:], cut[:half, half:]
        )
        out_ref[owners[k], :count, :] = product.astype(BF16)


def hidden_units(parts_ref, out_ref):
    members, total, width = parts_ref.shape
    count = total - SUM_ROWS
    half = width // 2
    product = parts_ref[0, :count, :].astype(F32)
    sums = parts_ref[0, count:, :].astype(F32)
    for k in range(1, members):
        product = product + parts_ref[k, :count, :].astype(F32)
        sums = sums + parts_ref[k, count:, :].astype(F32)
    row_sum = jnp.sum(jnp.transpose(sums), axis=1, keepdims=True)
    product = product * lax.rsqrt(row_sum / (members * 2 * width) + EPS)
    gate = product[:, :half]
    hidden = (gate * jax.nn.sigmoid(gate) * product[:, half:]).astype(BF16)
    for k in range(members):
        out_ref[k] = hidden


def last_product(member_ref, hidden_ref, *refs):
    *weight_refs, out_ref = refs
    members, _, width = hidden_ref.shape
    total = jnp.zeros((hidden_ref.shape[1], out_ref.shape[-1]), F32)
    for k, weight_ref in enumerate(weight_refs):
        owner = lax.rem(member_ref[0] + (members - k), members)
        total = total + dot(hidden_ref[owner], weight_ref[weight_ref.shape[0] - width :, :])
    out_ref[...] = total.astype(BF16).reshape(out_ref.shape)


def add_routed(back_ref, high_ref, low_ref, stream_ref, out_ref):
    back = back_ref[...].reshape(high_ref.shape[0], -1)
    routed = dot_on(high_ref[...], back, 0, 0) + dot_on(low_ref[...], back, 0, 0)
    out_ref[...] = (stream_ref[...].astype(F32) + routed).astype(BF16)


def body(
    tokens,
    conv_state,
    lru_state,
    mix_gain,
    input_weight,
    branch_weight,
    conv_taps,
    conv_bias,
    recur_weight,
    recur_bias,
    inject_weight,
    inject_bias,
    decay_param,
    output_weight,
    moe_gain,
    route_ids,
    route_logits,
    group_weight,
    expert_gate,
    expert_up,
    expert_down,
):
    seq_count, quarter = tokens.shape
    channels = lru_state.shape[1]
    members = lax.axis_size("tp")
    experts = lax.axis_size("ep")
    member = lax.axis_index("tp")
    place = member.astype(jnp.int32)[None]
    slots = experts * CAPACITY
    units = expert_gate.shape[2]

    token_parts = lax.all_to_all(
        jnp.broadcast_to(tokens[None], (members, *tokens.shape)), "tp", 0, 0, tiled=True
    )
    anywhere = pl.BlockSpec(memory_space=pl.ANY)
    operands = [
        mix_gain[None],
        input_weight,
        branch_weight,
        jnp.swapaxes(conv_state, 0, 1),
        conv_taps,
        conv_bias[None],
        recur_weight,
        recur_bias[None],
        inject_weight,
        inject_bias[None],
        decay_param[None],
        lru_state,
    ]
    half, whole = (quarter // 2, quarter), (quarter // 2 + units, quarter)
    cuts = [whole, whole, half, (units, quarter), half, (units, quarter)]
    ids = route_ids.T
    table = pltpu.VMEM((slots, seq_count), BF16)
    cutting = pl.pallas_call(
        functools.partial(cut_weights, members=members),
        out_shape=[jax.ShapeDtypeStruct(shape, BF16) for shape in cuts]
        + [pltpu.VMEM(value.shape, value.dtype) for value in operands]
        + [table],
        in_specs=[SMEM] + [anywhere] * (4 + len(operands)),
        out_specs=[anywhere] * len(cuts) + [VMEM] * (1 + len(operands)),
        scratch_shapes=[
            pltpu.VMEM((members, *whole), BF16),
            pltpu.VMEM(ids.shape, ids.dtype),
            pltpu.SemaphoreType.DMA((members, 5)),
            pltpu.SemaphoreType.DMA((len(cuts),)),
            pltpu.SemaphoreType.DMA((1 + len(operands),)),
        ],
    )
    loaded = cutting(place, ids, expert_gate, expert_up, expert_down, *operands)
    own, across, *sides = loaded[: len(cuts)]
    *operands, dispatch = [near(value) for value in loaded[len(cuts) :]]
    feature = member.astype(jnp.int32) * quarter
    combine_high, combine_low, gain_part = pl.pallas_call(
        combine_tables,
        out_shape=[table, table, pltpu.VMEM((1, quarter), F32)],
        in_specs=[SMEM] + [VMEM] * 3 + [anywhere],
        out_specs=[VMEM] * 3,
        scratch_shapes=[pltpu.SemaphoreType.DMA],
    )(feature[None], ids, route_logits.T, group_weight[None], moe_gain[None])
    copies, new_state, window = call(
        mixer,
        [
            pltpu.VMEM((members, seq_count, channels), BF16),
            jax.ShapeDtypeStruct((seq_count, channels), F32),
            jax.ShapeDtypeStruct((conv_state.shape[1], seq_count, channels), BF16),
        ],
        near(token_parts),
        *operands,
    )
    mixer_parts = lax.all_to_all(copies, "tp", 0, 0, tiled=True)

    def onward(value, step):
        ring = [(m, (m + step) % members) for m in range(members)]
        return lax.ppermute(value, "tp", ring)

    across = onward(across, 2)
    cut_next = onward(sides[0], 1)
    cut_last = onward(sides[2], 3)
    down_next = onward(sides[1], 1)
    down_last = onward(sides[3], 3)
    stream, outgoing = pl.pallas_call(
        stream_rows,
        out_shape=[
            pltpu.VMEM((seq_count, quarter), BF16),
            jax.ShapeDtypeStruct((experts, CAPACITY, quarter), BF16),
        ],
        in_specs=[VMEM] * 2 + [anywhere] * 2,
        out_specs=[VMEM] * 2,
        scratch_shapes=[
            pltpu.VMEM(output_weight.shape, BF16),
            pltpu.VMEM(tokens.shape, BF16),
            pltpu.SemaphoreType.DMA((members + 1,)),
        ],
    )(near(mixer_parts), dispatch, output_weight, tokens)

    arrived = lax.all_to_all(outgoing, "ep", 0, 0, tiled=True)
    arrived = arrived.reshape(slots, quarter)
    own, across = near(own), near(across)
    products = call(
        first_products,
        pltpu.VMEM((members, slots + SUM_ROWS, 2 * units), BF16),
        near(arrived),
        near(gain_part),
        own,
        near(cut_next),
        across,
        near(cut_last),
        scalar=place,
    )
    products = lax.all_to_all(products, "tp", 0, 0, tiled=True)
    hidden = call(hidden_units, pltpu.VMEM((members, slots, units), BF16), near(products))
    hidden, down_next, down_last = lax.optimization_barrier((hidden, down_next, down_last))
    hidden = lax.all_to_all(hidden, "tp", 0, 0, tiled=True)
    answer = call(
        last_product,
        pltpu.VMEM((experts, CAPACITY, quarter), BF16),
        near(hidden),
        own,
        near(down_next),
        across,
        near(down_last),
        scalar=place,
    )
    returned = lax.all_to_all(answer, "ep", 0, 0, tiled=True)
    result = call(
        add_routed,
        jax.ShapeDtypeStruct((seq_count, quarter), BF16),
        near(returned),
        near(combine_high),
        near(combine_low),
        near(stream),
    )
    return (result, new_state, jnp.swapaxes(window, 0, 1))


def solution(mesh):
    in_specs = (
        P("ep", "tp"),
        P("ep", None, "tp"),
        P("ep", "tp"),
        P(),
        P(None, "tp"),
        P(None, "tp"),
        P(None, "tp"),
        P("tp"),
        P("tp", None, None),
        P("tp"),
        P("tp", None, None),
        P("tp"),
        P("tp"),
        P(None, "tp"),
        P(),
        P("ep", None),
        P("ep", None),
        P("ep"),
        P("ep", None, "tp"),
        P("ep", None, "tp"),
        P("ep", "tp", None),
    )
    out_specs = (P("ep", "tp"), P("ep", "tp"), P("ep", None, "tp"))
    return jax.shard_map(body, mesh=mesh, in_specs=in_specs, out_specs=out_specs, check_vma=False)
```
